32 devices in a mesh: grp: 2 (over y), dp: 2 (over x), kv: 4 (over z), tp: 2 (over core).
Axes of the slice: x: 2, y: 2, z: 4, core: 2. Of those that a mesh axis runs over, the one named last changes fastest.
Arguments:
- tokens: bfloat16 [256, 4, 4096], P(('grp', 'dp'), None, ('kv', 'tp')), parts along dimension 0, may hold values from -160 to 160
- norm_gain: float32 [4096], replicated, may hold values from 0.1 to 1.9
- w_query: bfloat16 [4096, 16, 64], P(None, 'kv'), may hold values from -0.09375 to 0.09375
- w_key: bfloat16 [4096, 16, 64], P(None, 'kv'), may hold values from -0.09375 to 0.09375
- w_value: bfloat16 [4096, 16, 128], P(None, 'kv', 'tp'), may hold values from -0.09375 to 0.09375
- w_outgate: bfloat16 [4096, 16, 128], P(None, 'kv', 'tp'), may hold values from -0.09375 to 0.09375
- w_input: bfloat16 [4096, 16], replicated, may hold values from -0.09375 to 0.09375
- w_forget: bfloat16 [4096, 16], replicated, may hold values from -0.09375 to 0.09375
- forget_bias: float32 [16], replicated, may hold values from -1 to 4
- head_gain: float32 [16, 128], replicated, may hold values from 0.1 to 1.9
- w_out: bfloat16 [16, 128, 4096], P('kv', 'tp'), may hold values from -0.125 to 0.125
- memory: float32 [256, 16, 128, 64], P(('grp', 'dp'), 'kv', 'tp'), parts along dimension 0, may hold values from -12 to 12
- normalizer: float32 [256, 16, 64], P(('grp', 'dp'), 'kv'), parts along dimension 0, may hold values from -12 to 12
- stabilizer: float32 [256, 16], P(('grp', 'dp'), 'kv'), parts along dimension 0, may hold values from -1 to 1
- prev_keys: bfloat16 [256, 4, 16, 64], P(('grp', 'dp'), None, 'kv'), parts along dimension 0, may hold values from -6 to 6
- prev_values: bfloat16 [256, 4, 16, 128], P(('grp', 'dp'), None, 'kv', 'tp'), parts along dimension 0, may hold values from -6 to 6
- prev_input: float32 [256, 4, 16], P(('grp', 'dp'), None, 'kv'), parts along dimension 0, may hold values from -4 to 4
- prev_forget: float32 [256, 4, 16], P(('grp', 'dp'), None, 'kv'), parts along dimension 0, may hold values from -2 to -0.02
- accepted: int32 [256], P(('grp', 'dp')), parts along dimension 0, may hold values from 0 to 4
Outputs:
- mixed: bfloat16 [256, 4, 4096], P(('grp', 'dp'), None, ('kv', 'tp')), parts along dimension 0
- new_memory: float32 [256, 16, 128, 64], P(('grp', 'dp'), 'kv', 'tp'), parts along dimension 0
- new_normalizer: float32 [256, 16, 64], P(('grp', 'dp'), 'kv'), parts along dimension 0
- new_stabilizer: float32 [256, 16], P(('grp', 'dp'), 'kv'), parts along dimension 0
- new_keys: bfloat16 [256, 4, 16, 64], P(('grp', 'dp'), None, 'kv'), parts along dimension 0
- new_values: bfloat16 [256, 4, 16, 128], P(('grp', 'dp'), None, 'kv', 'tp'), parts along dimension 0
- new_input: float32 [256, 4, 16], P(('grp', 'dp'), None, 'kv'), parts along dimension 0
- new_forget: float32 [256, 4, 16], P(('grp', 'dp'), None, 'kv'), parts along dimension 0
The draws below stay inside these ranges and needn't reach their ends.
There are 2 independent parts, one for each index of `grp`. The reference program is written for one: setup_inputs(seed, part) draws one part's arguments, and reference() takes and returns one part's arrays. A program takes and returns all parts, laid end to end along the dimension named above; an argument that names none is the same for every part. Nothing has to cross between parts.
All inputs are finite; a program needn't handle non-finite values.
Results may differ from the reference program's by a relative error of at most 0.038.
Values may be sent and summed in bfloat16 or wider, within the bound.
A program may use at most 128 MiB of HBM per device.

```python
import math
import jax
import jax.numpy as jnp
from jax import lax

D = 4096
HEADS = 16
DK = 64
DV = 128
PROPOSALS = 4
SEQS = 128


def draw_tokens(key, part):
    base_key, row_key = jax.random.split(jax.random.fold_in(key, 17))
    position = jnp.arange(D, dtype=jnp.float32) / (D - 1)
    base = jnp.clip(jax.random.normal(base_key, (SEQS, PROPOSALS, D), jnp.float32), -4.0, 4.0)
    column = jnp.exp(math.log(3.0) * position)
    row_scale = jnp.exp(jax.random.uniform(row_key, (SEQS, PROPOSALS, 1), jnp.float32, 0.0, math.log(10.0)))
    return (base * column * row_scale).astype(jnp.bfloat16)


def with_ends(result, stream_key, low, largest):
    extent = result.shape
    place = [jax.random.randint(jax.random.fold_in(stream_key, axis), (), 0, extent[axis]) for axis in range(len(extent))]
    result = result.at[tuple(place)].set(low)
    longest = extent.index(max(extent))
    place[longest] = (place[longest] + 1) % extent[longest]
    return result.at[tuple(place)].set(largest)


def block_scale(own_key, shape, shards, least, high):
    def one(dim, shards_of):
        heights = jax.random.uniform(jax.random.fold_in(jax.random.fold_in(own_key, 6), dim), (shards_of,), jnp.float32, least / len(shards), high / len(shards))
        return jnp.repeat(jnp.exp(heights), shape[dim] // shards_of).reshape((-1,) + (1,) * (len(shape) - dim - 1))

    gain = one(*shards[0])
    for cut in shards[1:]:
        gain = gain * one(*cut)
    return gain


def bell_draw(key, extent, scale, reach, shards=(), kind=jnp.bfloat16):
    values = jax.random.normal(key, extent, jnp.float32) * scale
    if len(shards) > 0:
        values = block_scale(key, extent, shards, -0.22, 0.18) * values
    return jnp.clip(values, min=-reach, max=reach).astype(kind)


def setup_inputs(seed: int = 0, part: int = 0) -> dict:
    key_list = jax.random.split(jax.random.key(seed), 20)
    own_keys = jax.random.split(jax.random.fold_in(key_list[19], part), 20)
    tokens = draw_tokens(jax.random.fold_in(jax.random.fold_in(key_list[19], part), 71), part)
    norm_gain = jnp.clip(1.0 + 0.18 * jax.random.normal(key_list[1], (D,), jnp.float32), 0.1, 1.9)
    w_query = bell_draw(key_list[2], (D, HEADS, DK), D ** -0.5, 0.09375, ((1, 4),))
    w_key = bell_draw(key_list[3], (D, HEADS, DK), D ** -0.5, 0.09375, ((1, 4),))
    w_value = bell_draw(key_list[4], (D, HEADS, DV), D ** -0.5, 0.09375, ((1, 4), (2, 2)))
    w_outgate = bell_draw(key_list[5], (D, HEADS, DV), D ** -0.5, 0.09375, ((1, 4), (2, 2)))
    w_input = bell_draw(key_list[6], (D, HEADS), D ** -0.5, 0.09375)
    w_forget = bell_draw(key_list[7], (D, HEADS), D ** -0.5, 0.09375)
    forget_bias = jnp.clip(jax.random.uniform(key_list[8], (HEADS,), jnp.float32, -1.0, 4.0), -1.0, 4.0)
    head_gain = jnp.clip(1.0 + 0.18 * jax.random.normal(key_list[9], (HEADS, DV), jnp.float32), 0.1, 1.9)
    w_out = bell_draw(key_list[10], (HEADS, DV, D), (HEADS * DV) ** -0.5, 0.125, ((0, 4), (1, 2)))
    memory = bell_draw(own_keys[11], (SEQS, HEADS, DV, DK), 2.0, 12.0, ((0, 2), (1, 4), (2, 2)), jnp.float32)
    normalizer = bell_draw(own_keys[12], (SEQS, HEADS, DK), 2.0, 12.0, ((0, 2), (1, 4)), jnp.float32)
    stabilizer = jnp.clip(jax.random.uniform(own_keys[13], (SEQS, HEADS), jnp.float32, -1.0, 1.0) * block_scale(own_keys[13], (SEQS, HEADS), ((0, 2), (1, 4)), -0.4, 0.0), -1.0, 1.0)
    prev_keys = bell_draw(own_keys[14], (SEQS, PROPOSALS, HEADS, DK), 1.0, 6.0, ((0, 2), (2, 4)))
    prev_values = bell_draw(own_keys[15], (SEQS, PROPOSALS, HEADS, DV), 1.0, 6.0, ((0, 2), (2, 4), (3, 2)))
    prev_input = bell_draw(own_keys[16], (SEQS, PROPOSALS, HEADS), 1.0, 4.0, ((0, 2), (2, 4)), jnp.float32)
    prev_forget = jnp.clip(-2.0 + 1.98 * jax.random.uniform(own_keys[17], (SEQS, PROPOSALS, HEADS), jnp.float32) ** block_scale(own_keys[17], (SEQS, PROPOSALS, HEADS), ((0, 2), (2, 4)), -0.2, 0.2), -2.0, -0.02)
    accepted = with_ends(jax.random.randint(own_keys[18], (SEQS,), 0, PROPOSALS + 1), jax.random.fold_in(own_keys[18], 1), 0, PROPOSALS).astype(jnp.int32)
    return dict(tokens=tokens, norm_gain=norm_gain, w_query=w_query, w_key=w_key, w_value=w_value, w_outgate=w_outgate, w_input=w_input, w_forget=w_forget, forget_bias=forget_bias, head_gain=head_gain, w_out=w_out, memory=memory, normalizer=normalizer, stabilizer=stabilizer, prev_keys=prev_keys, prev_values=prev_values, prev_input=prev_input, prev_forget=prev_forget, accepted=accepted)


EPS = 1e-06
FAR_NEGATIVE = -1e+30
HIGHEST_PRECISION = lax.Precision.HIGHEST

def recurrent(query_f, key_all, value_all, gate_in, gate_forget, accepted, memory, normalizer, stabilizer):
    proposals = query_f.shape[1]
    total_span = key_all.shape[1]
    position = jnp.arange(total_span, dtype=jnp.int32)
    dropped = (position[None, :] < proposals) & (position[None, :] >= accepted[:, None])
    forget = jnp.where(dropped[:, :, None], 0.0, gate_forget)
    inflow = jnp.where(dropped[:, :, None], FAR_NEGATIVE, gate_in)
    running = jnp.cumsum(forget, axis=1)
    latest = running[:, proposals:]
    spread = latest[:, :, None, :] - running[:, None, :, :] + inflow[:, None, :, :]
    causal = position[None, :] <= (proposals + jnp.arange(proposals, dtype=jnp.int32))[:, None]
    spread = jnp.where(causal[None, :, :, None], spread, FAR_NEGATIVE)
    carried = latest + stabilizer[:, None, :]
    ceiling = jnp.maximum(lax.optimization_barrier(jnp.max(spread, axis=2)), carried)
    scores = jnp.einsum('sthk,suhk->stuh', query_f, key_all, precision=HIGHEST_PRECISION)
    weights = jnp.exp(spread - ceiling[:, :, None, :]) * scores
    carry_scale = jnp.exp(carried - ceiling)
    numerator = jnp.einsum('stuh,suhv->sthv', weights, value_all, precision=HIGHEST_PRECISION)
    numerator = numerator + carry_scale[..., None] * jnp.einsum('shvk,sthk->sthv', memory, query_f, precision=HIGHEST_PRECISION)
    denominator = lax.optimization_barrier(jnp.sum(weights, axis=2)) + carry_scale * jnp.einsum('shk,sthk->sth', normalizer, query_f, precision=HIGHEST_PRECISION)
    cell_out = numerator / jnp.maximum(jnp.abs(denominator), jnp.exp(-ceiling))[..., None]
    boundary = running[:, proposals - 1]
    reached = boundary[:, None, :] - running[:, :proposals] + inflow[:, :proposals]
    new_stabilizer = jnp.maximum(boundary + stabilizer, lax.optimization_barrier(jnp.max(reached, axis=1)))
    decay_old = jnp.exp(boundary + stabilizer - new_stabilizer)
    shares = jnp.exp(reached - new_stabilizer[:, None, :])
    new_memory = decay_old[:, :, None, None] * memory + jnp.einsum('sjh,sjhv,sjhk->shvk', shares, value_all[:, :proposals], key_all[:, :proposals], precision=HIGHEST_PRECISION)
    new_normalizer = decay_old[:, :, None] * normalizer + jnp.einsum('sjh,sjhk->shk', shares, key_all[:, :proposals], precision=HIGHEST_PRECISION)
    return (cell_out, new_memory, new_normalizer, new_stabilizer)

def project(normed, weight):
    return jnp.dot(normed, weight.reshape(weight.shape[0], -1), preferred_element_type=jnp.float32)

def reference(tokens, norm_gain, w_query, w_key, w_value, w_outgate, w_input, w_forget, forget_bias, head_gain, w_out, memory, normalizer, stabilizer, prev_keys, prev_values, prev_input, prev_forget, accepted):
    sequences, proposals, model_width = tokens.shape
    heads = w_query.shape[1]
    key_size = w_query.shape[2]
    value_size = w_value.shape[2]
    as_float = tokens.astype(jnp.float32)
    inv_scale = lax.rsqrt(lax.optimization_barrier(jnp.mean(as_float * as_float, axis=-1, keepdims=True)) + EPS)
    normed = (as_float * inv_scale * norm_gain).astype(jnp.bfloat16).reshape(sequences * proposals, model_width)
    queries = project(normed, w_query).astype(jnp.bfloat16).reshape(sequences, proposals, heads, key_size)
    new_keys = project(normed, w_key).astype(jnp.bfloat16).reshape(sequences, proposals, heads, key_size)
    new_values = project(normed, w_value).astype(jnp.bfloat16).reshape(sequences, proposals, heads, value_size)
    out_gate = project(normed, w_outgate).reshape(sequences, proposals, heads, value_size)
    new_input = project(normed, w_input).reshape(sequences, proposals, heads)
    new_forget = jax.nn.log_sigmoid(project(normed, w_forget).reshape(sequences, proposals, heads) + forget_bias)
    query_f = queries.astype(jnp.float32) * key_size ** (-0.5)
    key_all = jnp.concatenate([prev_keys, new_keys], axis=1).astype(jnp.float32)
    value_all = jnp.concatenate([prev_values, new_values], axis=1).astype(jnp.float32)
    gate_in = jnp.concatenate([prev_input, new_input], axis=1)
    gate_forget = jnp.concatenate([prev_forget, new_forget], axis=1)
    cell_out, new_memory, new_normalizer, new_stabilizer = recurrent(query_f, key_all, value_all, gate_in, gate_forget, accepted, memory, normalizer, stabilizer)
    squares = lax.optimization_barrier(jnp.mean(cell_out * cell_out, axis=-1, keepdims=True))
    gated = (jax.nn.sigmoid(out_gate) * cell_out * lax.rsqrt(squares + EPS) * head_gain).astype(jnp.bfloat16)
    mixed = jnp.dot(gated.reshape(sequences * proposals, heads * value_size), w_out.reshape(heads * value_size, model_width), preferred_element_type=jnp.float32)
    mixed = mixed.astype(jnp.bfloat16).reshape(sequences, proposals, model_width)
    return (mixed, new_memory, new_normalizer, new_stabilizer, new_keys, new_values, new_input, new_forget)
```

```python
import functools
import jax
import jax.numpy as jnp
from jax import lax
from jax.sharding import PartitionSpec as P
from jax.experimental import pallas as pl
from jax.experimental.pallas import tpu as pltpu

EPS = 1e-06
FAR_NEGATIVE = -1e30
HIGHEST = lax.Precision.HIGHEST
MESH = pl.DeviceIdType.MESH
F32 = jnp.float32
BF16 = jnp.bfloat16
VMEM_LIMIT = 60 << 20


def nn(a, b, precision=None):
    return lax.dot_general(
        a, b, (((1,), (0,)), ((), ())), precision=precision, preferred_element_type=F32
    )


def nt(a, b, precision=None):
    return lax.dot_general(
        a, b, (((1,), (1,)), ((), ())), precision=precision, preferred_element_type=F32
    )


def enter(n, z, c):
    barrier = pltpu.get_barrier_semaphore()
    pl.semaphore_signal(barrier, inc=1, device_id={"tp": 1 - c}, device_id_type=MESH)

    @pl.when(z > 0)
    def _():
        pl.semaphore_signal(barrier, inc=1, device_id={"kv": z - 1}, device_id_type=MESH)

    @pl.when(z < n - 1)
    def _():
        pl.semaphore_signal(barrier, inc=1, device_id={"kv": z + 1}, device_id_type=MESH)

    peers = 1 + (z > 0).astype(jnp.int32) + (z < n - 1).astype(jnp.int32)
    pl.semaphore_wait(barrier, peers)


def project_kernel(
    n, key_size,
    x_ref, gain_ref, wq_hbm, wk_hbm, wv_hbm, wo_hbm, wi_ref, wf_ref, bias_ref, out_hbm,
    q_out, k_out, v_out, og_out, gi_out, gf_out, wout_out,
    xg, wq, wk, wv, wo, q_acc, k_acc, v_acc, o_acc, gi_acc, gf_acc, ssr_acc, ssc_acc,
    load_sem, send_sem, recv_sem, wsend_sem, wrecv_sem,
):
    z = lax.axis_index("kv")
    c = lax.axis_index("tp")
    width = x_ref.shape[1]
    loads = [
        pltpu.make_async_copy(src, dst, load_sem.at[i])
        for i, (src, dst) in enumerate(((wq_hbm, wq), (wk_hbm, wk), (wv_hbm, wv), (wo_hbm, wo)))
    ]
    for load in loads:
        load.start()
    enter(n, z, c)
    mine = 2 * z + c

    def hop(src, slot, way, target):
        return pltpu.make_async_remote_copy(
            src_ref=src, dst_ref=xg.at[slot],
            send_sem=send_sem.at[way, slot], recv_sem=recv_sem.at[slot],
            device_id=target, device_id_type=MESH,
        )

    up, down, side = {"kv": z + 1}, {"kv": z - 1}, {"tp": 1 - c}

    @pl.when(z < n - 1)
    def _():
        hop(x_ref, mine, 0, up).start()

    @pl.when(z > 0)
    def _():
        hop(x_ref, mine, 1, down).start()

    hop(x_ref, mine, 2, side).start()

    rows_out = out_hbm.shape[0]

    def out_piece(i):
        col = pl.multiple_of((2 * i + 1 - c) * width, width)
        return pltpu.make_async_remote_copy(
            src_ref=out_hbm.at[:, pl.ds(col, width)],
            dst_ref=wout_out.at[i, pl.ds(rows_out, rows_out)],
            send_sem=wsend_sem.at[i], recv_sem=wrecv_sem.at[i],
            device_id=side, device_id_type=MESH,
        )

    def own_piece(i):
        col = pl.multiple_of((2 * i + c) * width, width)
        return pltpu.make_async_copy(
            out_hbm.at[:, pl.ds(col, width)], wout_out.at[i, pl.ds(0, rows_out)],
            load_sem.at[4 + i],
        )

    for i in range(n):
        out_piece(i).start()
        own_piece(i).start()

    for acc in (q_acc, k_acc, v_acc, o_acc, gi_acc, gf_acc, ssr_acc, ssc_acc):
        acc[...] = jnp.zeros_like(acc)
    for load in loads:
        load.wait()

    def process(src, slot):
        cols = pl.ds(pl.multiple_of(slot * width, width), width)
        x = src[...].astype(F32)
        xs = (x * gain_ref[:, cols]).astype(BF16)
        square = x * x
        high = square.astype(BF16)
        low = (square - high.astype(F32)).astype(BF16)
        ones_row = jnp.ones((8, width), BF16)
        ones_col = jnp.ones((k_acc.shape[1], width), BF16)
        ssr_acc[...] += nt(ones_row, high) + nt(ones_row, low)
        ssc_acc[...] += nt(high, ones_col) + nt(low, ones_col)
        q_acc[...] += nt(wq[:, cols], xs)
        k_acc[...] += nt(xs, wk[:, cols])
        v_acc[...] += nt(wv[:, cols], xs)
        o_acc[...] += nt(wo[:, cols], xs)
        gi_acc[...] += nt(wi_ref[:, cols], xs)
        gf_acc[...] += nt(wf_ref[:, cols], xs)

    process(x_ref, mine)

    def partner_block(owner):
        slot = 2 * owner + 1 - c
        hop(x_ref, slot, 2, side).wait_recv()
        process(xg.at[slot], slot)

    partner_block(z)

    def step(k, carry):
        @pl.when(z - k >= 0)
        def _():
            slot = 2 * (z - k) + c
            hop(x_ref, slot, 0, up).wait_recv()

            @pl.when(z < n - 1)
            def _():
                hop(xg.at[slot], slot, 0, up).start()

            hop(xg.at[slot], slot, 2, side).start()

        @pl.when(z + k <= n - 1)
        def _():
            slot = 2 * (z + k) + c
            hop(x_ref, slot, 1, down).wait_recv()

            @pl.when(z > 0)
            def _():
                hop(xg.at[slot], slot, 1, down).start()

            hop(xg.at[slot], slot, 2, side).start()

        @pl.when(z - k >= 0)
        def _():
            slot = 2 * (z - k) + c
            process(xg.at[slot], slot)
            partner_block(z - k)

        @pl.when(z + k <= n - 1)
        def _():
            slot = 2 * (z + k) + c
            process(xg.at[slot], slot)
            partner_block(z + k)

        return carry

    lax.fori_loop(1, n, step, 0)

    inv_row = lax.rsqrt(ssr_acc[0:1] / gain_ref.shape[1] + EPS)
    inv_col = lax.rsqrt(ssc_acc[...] / gain_ref.shape[1] + EPS)
    q_out[...] = ((q_acc[...] * inv_row).astype(BF16).astype(F32) * key_size ** (-0.5)).astype(BF16)
    k_out[...] = (k_acc[...] * inv_col).astype(BF16)
    v_out[...] = (v_acc[...] * inv_row).astype(BF16)
    og_out[...] = o_acc[...] * inv_row
    all_heads = gf_acc.shape[0]
    diagonal = lax.broadcasted_iota(jnp.int32, (all_heads, all_heads), 0) == (
        lax.broadcasted_iota(jnp.int32, (all_heads, all_heads), 1)
    )
    shift = nn(jnp.where(diagonal, bias_ref[...], 0.0), jnp.ones(gf_acc.shape, F32), HIGHEST)
    gi_acc[...] = gi_acc[...] * inv_row
    raw = gf_acc[...] * inv_row + shift
    gf_acc[...] = jnp.minimum(raw, 0.0) - jnp.log1p(jnp.exp(-jnp.abs(raw)))
    local_heads = gi_out.shape[0]
    for acc, out in ((gi_acc, gi_out), (gf_acc, gf_out)):
        total = acc[:local_heads]
        for i in range(1, n):
            total = jnp.where(z == i, acc[i * local_heads : (i + 1) * local_heads], total)
        out[...] = total

    for i in range(n):
        own_piece(i).wait()
        out_piece(i).wait()

    def drain(i, carry):
        slot = 2 * i + c

        @pl.when((i <= z) & (z < n - 1))
        def _():
            hop(x_ref, slot, 0, up).wait_send()

        @pl.when((i >= z) & (z > 0))
        def _():
            hop(x_ref, slot, 1, down).wait_send()

        hop(x_ref, slot, 2, side).wait_send()
        return carry

    lax.fori_loop(0, n, drain, 0)


def recurrent_kernel(
    q_ref, k_ref, v_ref, og_ref, gi_ref, gf_ref, pk_ref, pv_ref, pi_ref, pf_ref,
    acc_ref, stab_ref, nrm_ref, gain_ref, mem_ref,
    nm_ref, nn_ref, ns_ref, ni_ref, nf_ref, g_ref, sq_ref,
    vts, kps, dfull, wexp, ro,
):
    step = pl.program_id(0)
    steps = pl.num_programs(0)
    block, heads, values, keys = mem_ref.shape
    span, _, seqs = pi_ref.shape
    rows = seqs * span
    lanes = 128
    iota = lambda shape, d: lax.broadcasted_iota(jnp.int32, shape, d)

    @pl.when(step == 0)
    def _():
        spread = (iota((seqs, rows), 0) == iota((seqs, rows), 1) // span)
        expand = spread.astype(F32)
        lane_pos = iota((span, rows), 1) % span == iota((span, rows), 0)
        eye = iota((seqs, seqs), 0) == iota((seqs, seqs), 1)
        dropped = iota((span, seqs), 0) >= acc_ref[...]
        ro[...] = jnp.zeros_like(ro)
        for h in range(heads):
            stab = stab_ref[h : h + 1, :]
            f = jnp.where(dropped, 0.0, pf_ref[:, h, :])
            i = jnp.where(dropped, FAR_NEGATIVE, pi_ref[:, h, :])
            new_i = nt(jnp.where(lane_pos, gi_ref[h : h + 1, :], 0.0), expand, HIGHEST)
            new_f = nt(jnp.where(lane_pos, gf_ref[h : h + 1, :], 0.0), expand, HIGHEST)
            ni_ref[:, h, :] = new_i
            nf_ref[:, h, :] = new_f
            total = []
            for j in range(span):
                total.append(f[j : j + 1] + total[-1] if total else f[0:1])
            e = total[-1]
            for j in range(span):
                total.append(total[-1] + new_f[j : j + 1])
            run_prev = jnp.concatenate(total[:span], axis=0)
            run_all = jnp.concatenate(total, axis=0)
            in_all = jnp.concatenate([i, new_i], axis=0)
            u = e - run_prev + i
            ns = jnp.maximum(e + stab, jnp.max(u, axis=0, keepdims=True))
            ns_ref[h : h + 1, :] = ns
            decay = jnp.exp(e + stab - ns)
            shares = jnp.exp(u - ns)
            share_row = jnp.sum(
                jnp.where(lane_pos, nn(shares, expand, HIGHEST), 0.0), axis=0, keepdims=True
            )
            kps[h] = pk_ref[:, h * keys : (h + 1) * keys]
            part = slice(h * values, (h + 1) * values)
            vts[part, :] = (pv_ref[part, :].astype(F32) * share_row).astype(BF16)
            full = nn(jnp.where(eye, decay, 0.0), jnp.ones((seqs, keys), F32), HIGHEST)
            dfull[h] = full
            mixed = jnp.where(spread, share_row, 0.0).astype(BF16)
            nn_ref[:, h, :] = full * nrm_ref[:, h, :] + nn(mixed, kps[h])
            gathered = jnp.zeros((16, rows), F32)
            position = iota((2 * span, seqs), 0)
            for t in range(span):
                latest = total[span + t]
                d = jnp.where(position <= span + t, latest - run_all + in_all, FAR_NEGATIVE)
                g = latest + stab
                top = jnp.maximum(jnp.max(d, axis=0, keepdims=True), g)
                pad = jnp.zeros((16 - 2 * span - 2, seqs), F32)
                stack = jnp.concatenate(
                    [jnp.exp(d - top), jnp.exp(g - top), jnp.exp(-top), pad], axis=0
                )
                wide = nn(stack, expand, HIGHEST)
                gathered = jnp.where(iota((16, rows), 1) % span == t, wide, gathered)
            wexp[h] = gathered

    first = step * block
    start = pl.multiple_of((first * span) // lanes * lanes, lanes)
    half = pl.ds(start, lanes)
    seq = (iota((values, lanes), 1) + start) // span - first
    for h in range(heads):
        part = slice(h * values, (h + 1) * values)
        memory = [mem_ref[s, h] for s in range(block)]
        packed = jnp.concatenate([m.astype(BF16) for m in memory], axis=0)
        read = nn(packed, q_ref[h * keys : (h + 1) * keys, half])
        total = ro[part, half]
        for s in range(block):
            total = jnp.where(seq == s, read[s * values : (s + 1) * values], total)
        ro[part, half] = total
        shared = vts[part, half]
        zero = jnp.zeros_like(shared)
        left = jnp.concatenate([jnp.where(seq == s, shared, zero) for s in range(block)], axis=0)
        update = nn(left, kps[h, half, :])
        for s in range(block):
            nm_ref[s, h] = (
                dfull[h, pl.ds(first + s, 1), :] * memory[s]
                + update[s * values : (s + 1) * values]
            )

    @pl.when(step == steps - 1)
    def _():
        same = iota((rows, rows), 0) // span == iota((rows, rows), 1) // span
        spread = iota((seqs, rows), 0) == iota((seqs, rows), 1) // span
        eye = iota((values, values), 0) == iota((values, values), 1)
        q = q_ref[...]
        owner = iota(q.shape, 0) // keys

        def tile(w):
            w = jnp.concatenate([w] * (8 // span), axis=0)
            return jnp.broadcast_to(w[None], (rows // 8, 8, rows)).reshape(rows, rows)

        for h in range(heads):
            part = slice(h * values, (h + 1) * values)
            only = jnp.where(owner == h, q, jnp.zeros_like(q))
            w = wexp[h]
            w_prev = jnp.where(same, tile(w[:span]) * nn(pk_ref[...], only), 0.0)
            w_new = jnp.where(same, tile(w[span : 2 * span]) * nn(k_ref[...], only), 0.0)
            carry = w[2 * span : 2 * span + 1]
            floor = w[2 * span + 1 : 2 * span + 2]
            top = nn(pv_ref[part, :], w_prev.astype(BF16)) + nn(v_ref[part, :], w_new.astype(BF16))
            top = top + carry * ro[part, :]
            nq = nn(nrm_ref[:, h, :].astype(BF16), q_ref[h * keys : (h + 1) * keys, :])
            nq = jnp.sum(jnp.where(spread, nq, 0.0), axis=0, keepdims=True)
            under = jnp.sum(w_prev + w_new, axis=0, keepdims=True) + carry * nq
            cell = top / jnp.maximum(jnp.abs(under), floor)
            sq_ref[h : h + 1, :] = jnp.sum(cell * cell, axis=0, keepdims=True)
            gain = nn(
                jnp.where(eye, gain_ref[h : h + 1, :], 0.0), jnp.ones((values, rows), F32), HIGHEST
            )
            g_ref[part, :] = (jax.nn.sigmoid(og_ref[part, :]) * cell * gain).astype(BF16)


def output_kernel(
    n, full_values,
    g_ref, sq_ref, w_ref,
    y_ref,
    g_in, sq_in, both, from_low, from_high, to_high, to_low,
    side_send, side_recv, up_send, up_recv, down_send, down_recv,
):
    z = lax.axis_index("kv")
    c = lax.axis_index("tp")
    enter(n, z, c)
    side = {"tp": 1 - c}
    swaps = [
        pltpu.make_async_remote_copy(
            src_ref=src, dst_ref=dst, send_sem=side_send.at[i], recv_sem=side_recv.at[i],
            device_id=side, device_id_type=MESH,
        )
        for i, (src, dst) in enumerate(((g_ref, g_in), (sq_ref, sq_in)))
    ]
    for swap in swaps:
        swap.start()
    for swap in swaps:
        swap.wait_recv()
    inv = lax.rsqrt((sq_ref[...] + sq_in[...]) / full_values + EPS)
    channels = g_ref.shape[0]
    heads = sq_ref.shape[0]
    values = channels // heads
    for i, src in enumerate((g_ref, g_in)):
        scaled = jnp.concatenate(
            [
                src[h * values : (h + 1) * values, :].astype(F32) * inv[h : h + 1, :]
                for h in range(heads)
            ],
            axis=0,
        )
        both[:, i * channels : (i + 1) * channels] = scaled.T.astype(BF16)

    def partial(d):
        return nn(both[...], w_ref[d])

    def upward(d):
        return pltpu.make_async_remote_copy(
            src_ref=to_high.at[d], dst_ref=from_low.at[d],
            send_sem=up_send.at[d], recv_sem=up_recv.at[d],
            device_id={"kv": z + 1}, device_id_type=MESH,
        )

    def downward(d):
        return pltpu.make_async_remote_copy(
            src_ref=to_low.at[d], dst_ref=from_high.at[d],
            send_sem=down_send.at[d], recv_sem=down_recv.at[d],
            device_id={"kv": z - 1}, device_id_type=MESH,
        )

    def step(i, carry):
        high = n - i
        low = i - 1

        @pl.when(high > z)
        def _():
            to_high[high] = partial(high).astype(BF16)

            @pl.when(z > 0)
            def _():
                upward(high).wait_recv()
                to_high[high] = (
                    to_high[high].astype(F32) + from_low[high].astype(F32)
                ).astype(BF16)

            upward(high).start()

        @pl.when(low < z)
        def _():
            to_low[low] = partial(low).astype(BF16)

            @pl.when(z < n - 1)
            def _():
                downward(low).wait_recv()
                to_low[low] = (
                    to_low[low].astype(F32) + from_high[low].astype(F32)
                ).astype(BF16)

            downward(low).start()

        return carry

    lax.fori_loop(1, n, step, 0)
    total = partial(z)
    y_ref[...] = total.astype(BF16)

    @pl.when(z == 0)
    def _():
        downward(z).wait_recv()
        y_ref[...] = (partial(z) + from_high[z].astype(F32)).astype(BF16)

    @pl.when(z == n - 1)
    def _():
        upward(z).wait_recv()
        y_ref[...] = (partial(z) + from_low[z].astype(F32)).astype(BF16)

    @pl.when((z > 0) & (z < n - 1))
    def _():
        upward(z).wait_recv()
        downward(z).wait_recv()
        y_ref[...] = (
            partial(z) + from_low[z].astype(F32) + from_high[z].astype(F32)
        ).astype(BF16)

    def drain(i, carry):
        @pl.when(n - i > z)
        def _():
            upward(n - i).wait_send()

        @pl.when(i - 1 < z)
        def _():
            downward(i - 1).wait_send()

        return carry

    lax.fori_loop(1, n, drain, 0)
    for swap in swaps:
        swap.wait_send()


def shards(
    n, tokens, norm_gain, w_query, w_key, w_value, w_outgate, w_input, w_forget, forget_bias,
    head_gain, w_out, memory, normalizer, stabilizer, prev_keys, prev_values, prev_input,
    prev_forget, accepted,
):
    seqs, span, width = tokens.shape
    depth, heads, keys = w_query.shape
    values = w_value.shape[2]
    rows = seqs * span
    hk, hv = heads * keys, heads * values
    all_heads = w_input.shape[1]
    sds = jax.ShapeDtypeStruct
    vm = pl.BlockSpec(memory_space=pltpu.VMEM)
    hbm = pl.BlockSpec(memory_space=pl.ANY)
    flip = lambda w: w.transpose(1, 2, 0).reshape(-1, depth)

    q, k, v, og, gi, gf, wout = pl.pallas_call(
        functools.partial(project_kernel, n, keys),
        out_shape=[
            sds((hk, rows), BF16), sds((rows, hk), BF16), sds((hv, rows), BF16),
            sds((hv, rows), F32), sds((heads, rows), F32), sds((heads, rows), F32),
            sds((n, 2 * hv, width), BF16),
        ],
        in_specs=[vm, vm, hbm, hbm, hbm, hbm, vm, vm, vm, hbm],
        out_specs=[vm] * 6 + [vm],
        scratch_shapes=[
            pltpu.VMEM((2 * n, rows, width), BF16),
            pltpu.VMEM((hk, depth), BF16), pltpu.VMEM((hk, depth), BF16),
            pltpu.VMEM((hv, depth), BF16), pltpu.VMEM((hv, depth), BF16),
            pltpu.VMEM((hk, rows), F32), pltpu.VMEM((rows, hk), F32),
            pltpu.VMEM((hv, rows), F32), pltpu.VMEM((hv, rows), F32),
            pltpu.VMEM((all_heads, rows), F32), pltpu.VMEM((all_heads, rows), F32),
            pltpu.VMEM((8, rows), F32), pltpu.VMEM((rows, hk), F32),
            pltpu.SemaphoreType.DMA((4 + n,)),
            pltpu.SemaphoreType.DMA((3, 2 * n)),
            pltpu.SemaphoreType.DMA((2 * n,)),
            pltpu.SemaphoreType.DMA((n,)),
            pltpu.SemaphoreType.DMA((n,)),
        ],
        compiler_params=pltpu.CompilerParams(
            collective_id=0, has_side_effects=True, vmem_limit_bytes=VMEM_LIMIT
        ),
        name="project",
    )(
        tokens.reshape(rows, width), norm_gain.reshape(1, depth),
        flip(w_query), flip(w_key), flip(w_value), flip(w_outgate),
        w_input.T, w_forget.T, forget_bias.reshape(1, all_heads), w_out.reshape(hv, -1),
    )

    gain_block = lax.dynamic_slice(
        head_gain,
        (lax.axis_index("kv") * heads, lax.axis_index("tp") * values),
        (heads, values),
    )
    block = 8
    whole = lambda *shape: pl.BlockSpec(shape, lambda i: (0,) * len(shape))
    tile = pl.BlockSpec((block, heads, values, keys), lambda i: (i, 0, 0, 0))
    new_memory, new_normalizer, ns, ni, nf, g, sq = pl.pallas_call(
        recurrent_kernel,
        grid=(seqs // block,),
        out_shape=[
            sds(memory.shape, F32), sds(normalizer.shape, F32), sds((heads, seqs), F32),
            sds((span, heads, seqs), F32), sds((span, heads, seqs), F32),
            sds((hv, rows), BF16), sds((heads, rows), F32),
        ],
        in_specs=[
            whole(hk, rows), whole(rows, hk), whole(hv, rows), whole(hv, rows),
            whole(heads, rows), whole(heads, rows), whole(rows, hk), whole(hv, rows),
            whole(span, heads, seqs), whole(span, heads, seqs), whole(1, seqs),
            whole(heads, seqs), whole(seqs, heads, keys), whole(heads, values), tile,
        ],
        out_specs=[
            tile, whole(seqs, heads, keys), whole(heads, seqs), whole(span, heads, seqs),
            whole(span, heads, seqs), whole(hv, rows), whole(heads, rows),
        ],
        scratch_shapes=[
            pltpu.VMEM((hv, rows), BF16), pltpu.VMEM((heads, rows, keys), BF16),
            pltpu.VMEM((heads, seqs, keys), F32), pltpu.VMEM((heads, 16, rows), F32),
            pltpu.VMEM((hv, rows), F32),
        ],
        compiler_params=pltpu.CompilerParams(vmem_limit_bytes=VMEM_LIMIT),
        name="recurrent",
    )(
        q, k, v, og, gi, gf, prev_keys.reshape(rows, hk),
        prev_values.reshape(rows, hv).T,
        prev_input.transpose(1, 2, 0), prev_forget.transpose(1, 2, 0),
        accepted.reshape(1, seqs), stabilizer.T, normalizer, gain_block, memory,
    )

    y = pl.pallas_call(
        functools.partial(output_kernel, n, values * 2),
        out_shape=sds((rows, width), BF16),
        in_specs=[vm] * 3,
        out_specs=vm,
        scratch_shapes=[
            pltpu.VMEM((hv, rows), BF16), pltpu.VMEM((heads, rows), F32),
            pltpu.VMEM((rows, 2 * hv), BF16),
            pltpu.VMEM((n, rows, width), BF16), pltpu.VMEM((n, rows, width), BF16),
            pltpu.VMEM((n, rows, width), BF16), pltpu.VMEM((n, rows, width), BF16),
            pltpu.SemaphoreType.DMA((2,)), pltpu.SemaphoreType.DMA((2,)),
            pltpu.SemaphoreType.DMA((n,)), pltpu.SemaphoreType.DMA((n,)),
            pltpu.SemaphoreType.DMA((n,)), pltpu.SemaphoreType.DMA((n,)),
        ],
        compiler_params=pltpu.CompilerParams(
            collective_id=1, has_side_effects=True, vmem_limit_bytes=VMEM_LIMIT
        ),
        name="output",
    )(g, sq, wout)

    return (
        y.reshape(seqs, span, width),
        new_memory,
        new_normalizer,
        ns.T,
        k.reshape(seqs, span, heads, keys),
        v.T.reshape(seqs, span, heads, values),
        ni.transpose(2, 0, 1),
        nf.transpose(2, 0, 1),
    )


def solution(mesh):
    return jax.shard_map(
        functools.partial(shards, mesh.shape["kv"]),
        mesh=mesh,
        in_specs=(
            P(("grp", "dp"), None, ("kv", "tp")),
            P(),
            P(None, "kv", None),
            P(None, "kv", None),
            P(None, "kv", "tp"),
            P(None, "kv", "tp"),
            P(),
            P(),
            P(),
            P(),
            P("kv", "tp", None),
            P(("grp", "dp"), "kv", "tp", None),
            P(("grp", "dp"), "kv", None),
            P(("grp", "dp"), "kv"),
            P(("grp", "dp"), None, "kv", None),
            P(("grp", "dp"), None, "kv", "tp"),
            P(("grp", "dp"), None, "kv"),
            P(("grp", "dp"), None, "kv"),
            P(("grp", "dp")),
        ),
        out_specs=(
            P(("grp", "dp"), None, ("kv", "tp")),
            P(("grp", "dp"), "kv", "tp", None),
            P(("grp", "dp"), "kv", None),
            P(("grp", "dp"), "kv"),
            P(("grp", "dp"), None, "kv", None),
            P(("grp", "dp"), None, "kv", "tp"),
            P(("grp", "dp"), None, "kv"),
            P(("grp", "dp"), None, "kv"),
        ),
        check_vma=False,
    )
```

```python
import functools
import jax
import jax.numpy as jnp
from jax import lax
from jax.sharding import PartitionSpec as P
from jax.experimental import pallas as pl
from jax.experimental.pallas import tpu as pltpu

EPS = 1e-06
FAR_NEGATIVE = -1e30
HIGHEST = lax.Precision.HIGHEST
MESH = pl.DeviceIdType.MESH
F32 = jnp.float32
BF16 = jnp.bfloat16
VMEM_LIMIT = 60 << 20


def nn(a, b, precision=None):
    return lax.dot_general(
        a, b, (((1,), (0,)), ((), ())), precision=precision, preferred_element_type=F32
    )


def nt(a, b, precision=None):
    return lax.dot_general(
        a, b, (((1,), (1,)), ((), ())), precision=precision, preferred_element_type=F32
    )


def enter(n, z, c):
    barrier = pltpu.get_barrier_semaphore()
    pl.semaphore_signal(barrier, inc=1, device_id={"tp": 1 - c}, device_id_type=MESH)

    @pl.when(z > 0)
    def _():
        pl.semaphore_signal(barrier, inc=1, device_id={"kv": z - 1}, device_id_type=MESH)

    @pl.when(z < n - 1)
    def _():
        pl.semaphore_signal(barrier, inc=1, device_id={"kv": z + 1}, device_id_type=MESH)

    peers = 1 + (z > 0).astype(jnp.int32) + (z < n - 1).astype(jnp.int32)
    pl.semaphore_wait(barrier, peers)


def project_kernel(
    n, key_size, halves,
    x_ref, gain_ref, wq_hbm, wk_hbm, wv_hbm, wo_hbm, wi_hbm, wf_hbm, bias_ref, out_hbm,
    q_out, k_out, v_out, og_out, gi_out, gf_out, wout_out,
    xg, weights, acc, squares,
    load_sem, own_sem, send_sem, recv_sem, wsend_sem, wrecv_sem,
):
    z = lax.axis_index("kv")
    c = lax.axis_index("tp")
    width = x_ref.shape[2]
    rows = x_ref.shape[0] * x_ref.shape[1]
    height = rows // halves
    loads, spans, at = [], [], 0
    for i, src in enumerate((wq_hbm, wk_hbm, wv_hbm, wo_hbm, wi_hbm, wf_hbm)):
        size = src.shape[0]
        spans.append(slice(at, at + size))
        loads.append(
            pltpu.make_async_copy(src, weights.at[pl.ds(at, size)], load_sem.at[i])
        )
        at += size
    for load in loads:
        load.start()
    mine = 2 * z + c
    flat = x_ref[...].reshape(rows, width)
    for half in range(halves):
        xg[mine, half] = flat[half * height : (half + 1) * height]
    acc[...] = jnp.zeros_like(acc)
    squares[...] = jnp.zeros_like(squares)
    enter(n, z, c)

    def hop(slot, half, way, target):
        return pltpu.make_async_remote_copy(
            src_ref=xg.at[slot, half], dst_ref=xg.at[slot, half],
            send_sem=send_sem.at[way, slot, half], recv_sem=recv_sem.at[slot, half],
            device_id=target, device_id_type=MESH,
        )

    up, down, side = {"kv": z + 1}, {"kv": z - 1}, {"tp": 1 - c}

    for half in range(halves):
        @pl.when(z < n - 1)
        def _():
            hop(mine, half, 0, up).start()

        @pl.when(z > 0)
        def _():
            hop(mine, half, 1, down).start()

        hop(mine, half, 2, side).start()

    rows_out = out_hbm.shape[0]

    def out_piece(i):
        col = pl.multiple_of((2 * i + 1 - c) * width, width)
        return pltpu.make_async_remote_copy(
            src_ref=out_hbm.at[:, pl.ds(col, width)],
            dst_ref=wout_out.at[i, pl.ds(rows_out, rows_out)],
            send_sem=wsend_sem.at[i], recv_sem=wrecv_sem.at[i],
            device_id=side, device_id_type=MESH,
        )

    def own_piece(i):
        col = pl.multiple_of((2 * i + c) * width, width)
        return pltpu.make_async_copy(
            out_hbm.at[:, pl.ds(col, width)], wout_out.at[i, pl.ds(0, rows_out)],
            own_sem.at[i],
        )

    for i in range(n):
        out_piece(i).start()
        own_piece(i).start()
    for load in loads:
        load.wait()

    def process(slot):
        cols = pl.ds(pl.multiple_of(slot * width, width), width)
        x = jnp.concatenate([xg[slot, half] for half in range(halves)], axis=0).astype(F32)
        square = x * x
        total = squares[...]
        for i in range(width // 128):
            total = total + square[:, i * 128 : (i + 1) * 128]
        squares[...] = total
        acc[...] += nt(weights[:, cols], (x * gain_ref[:, cols]).astype(BF16))

    def process_owner(owner):
        process(2 * owner + c)
        slot = 2 * owner + 1 - c
        for half in range(halves):
            hop(slot, half, 2, side).wait_recv()
        process(slot)

    def forward(k, half):
        @pl.when(z - k >= 0)
        def _():
            slot = 2 * (z - k) + c
            hop(slot, half, 0, up).wait_recv()

            @pl.when(z < n - 1)
            def _():
                hop(slot, half, 0, up).start()

            hop(slot, half, 2, side).start()

        @pl.when(z + k <= n - 1)
        def _():
            slot = 2 * (z + k) + c
            hop(slot, half, 1, down).wait_recv()

            @pl.when(z > 0)
            def _():
                hop(slot, half, 1, down).start()

            hop(slot, half, 2, side).start()

    def step(k, carry):
        for half in range(halves - 1):
            forward(k, half)

        @pl.when(z - (k - 1) >= 0)
        def _():
            process_owner(z - (k - 1))

        forward(k, halves - 1)

        @pl.when((z + k - 1 <= n - 1) & (k > 1))
        def _():
            process_owner(z + k - 1)

        return carry

    lax.fori_loop(1, n + 1, step, 0)

    depth = gain_ref.shape[1]
    total = nt(jnp.ones((8, 128), F32), squares[...], HIGHEST)
    inv = lax.rsqrt(total[0:1] / depth + EPS)
    q, k, v, og, gi, gf = [acc[part, :] * inv for part in spans]
    q_out[...] = (q.astype(BF16).astype(F32) * key_size ** (-0.5)).astype(BF16)
    k_out[...] = k.T.astype(BF16)
    v_out[...] = v.astype(BF16)
    og_out[...] = og
    all_heads = gf.shape[0]
    diagonal = lax.broadcasted_iota(jnp.int32, (all_heads, all_heads), 0) == (
        lax.broadcasted_iota(jnp.int32, (all_heads, all_heads), 1)
    )
    shift = nn(jnp.where(diagonal, bias_ref[...], 0.0), jnp.ones(gf.shape, F32), HIGHEST)
    raw = gf + shift
    gf = jnp.minimum(raw, 0.0) - jnp.log1p(jnp.exp(-jnp.abs(raw)))
    local_heads = gi_out.shape[0]
    for values, out in ((gi, gi_out), (gf, gf_out)):
        total = values[:local_heads]
        for i in range(1, n):
            total = jnp.where(z == i, values[i * local_heads : (i + 1) * local_heads], total)
        out[...] = total

    for i in range(n):
        own_piece(i).wait()
        out_piece(i).wait()

    def drain(i, carry):
        slot = 2 * i + c
        for half in range(halves):
            @pl.when((i <= z) & (z < n - 1))
            def _():
                hop(slot, half, 0, up).wait_send()

            @pl.when((i >= z) & (z > 0))
            def _():
                hop(slot, half, 1, down).wait_send()

            hop(slot, half, 2, side).wait_send()
        return carry

    lax.fori_loop(0, n, drain, 0)


def recurrent_kernel(
    q_ref, k_ref, v_ref, og_ref, gi_ref, gf_ref, pk_ref, pv_ref, pi_ref, pf_ref,
    acc_ref, stab_ref, nrm_ref, gain_ref, mem_ref,
    nm_ref, nn_ref, ns_ref, ni_ref, nf_ref, g_ref, sq_ref,
    vts, kps, dfull, wexp, ro,
):
    step = pl.program_id(0)
    steps = pl.num_programs(0)
    block, heads, values, keys = mem_ref.shape
    span, _, seqs = pi_ref.shape
    rows = seqs * span
    lanes = 128
    iota = lambda shape, d: lax.broadcasted_iota(jnp.int32, shape, d)

    @pl.when(step == 0)
    def _():
        spread = (iota((seqs, rows), 0) == iota((seqs, rows), 1) // span)
        expand = spread.astype(F32)
        lane_pos = iota((span, rows), 1) % span == iota((span, rows), 0)
        eye = iota((seqs, seqs), 0) == iota((seqs, seqs), 1)
        dropped = iota((span, seqs), 0) >= acc_ref[...]
        ro[...] = jnp.zeros_like(ro)
        for h in range(heads):
            stab = stab_ref[h : h + 1, :]
            f = jnp.where(dropped, 0.0, pf_ref[:, h, :])
            i = jnp.where(dropped, FAR_NEGATIVE, pi_ref[:, h, :])
            new_i = nt(jnp.where(lane_pos, gi_ref[h : h + 1, :], 0.0), expand, HIGHEST)
            new_f = nt(jnp.where(lane_pos, gf_ref[h : h + 1, :], 0.0), expand, HIGHEST)
            ni_ref[:, h, :] = new_i
            nf_ref[:, h, :] = new_f
            total = []
            for j in range(span):
                total.append(f[j : j + 1] + total[-1] if total else f[0:1])
            e = total[-1]
            for j in range(span):
                total.append(total[-1] + new_f[j : j + 1])
            run_prev = jnp.concatenate(total[:span], axis=0)
            run_all = jnp.concatenate(total, axis=0)
            in_all = jnp.concatenate([i, new_i], axis=0)
            u = e - run_prev + i
            ns = jnp.maximum(e + stab, jnp.max(u, axis=0, keepdims=True))
            ns_ref[h : h + 1, :] = ns
            decay = jnp.exp(e + stab - ns)
            shares = jnp.exp(u - ns)
            share_row = jnp.sum(
                jnp.where(lane_pos, nn(shares, expand, HIGHEST), 0.0), axis=0, keepdims=True
            )
            kps[h] = pk_ref[:, h * keys : (h + 1) * keys]
            part = slice(h * values, (h + 1) * values)
            vts[part, :] = (pv_ref[part, :].astype(F32) * share_row).astype(BF16)
            full = nn(jnp.where(eye, decay, 0.0), jnp.ones((seqs, keys), F32), HIGHEST)
            dfull[h] = full
            mixed = jnp.where(spread, share_row, 0.0).astype(BF16)
            nn_ref[:, h, :] = full * nrm_ref[:, h, :] + nn(mixed, kps[h])
            gathered = jnp.zeros((16, rows), F32)
            position = iota((2 * span, seqs), 0)
            for t in range(span):
                latest = total[span + t]
                d = jnp.where(position <= span + t, latest - run_all + in_all, FAR_NEGATIVE)
                g = latest + stab
                top = jnp.maximum(jnp.max(d, axis=0, keepdims=True), g)
                pad = jnp.zeros((16 - 2 * span - 2, seqs), F32)
                stack = jnp.concatenate(
                    [jnp.exp(d - top), jnp.exp(g - top), jnp.exp(-top), pad], axis=0
                )
                wide = nn(stack, expand, HIGHEST)
                gathered = jnp.where(iota((16, rows), 1) % span == t, wide, gathered)
            wexp[h] = gathered

    first = step * block
    start = pl.multiple_of((first * span) // lanes * lanes, lanes)
    half = pl.ds(start, lanes)
    seq = (iota((values, lanes), 1) + start) // span - first
    for h in range(heads):
        part = slice(h * values, (h + 1) * values)
        memory = [mem_ref[s, h] for s in range(block)]
        packed = jnp.concatenate([m.astype(BF16) for m in memory], axis=0)
        read = nn(packed, q_ref[h * keys : (h + 1) * keys, half])
        total = ro[part, half]
        for s in range(block):
            total = jnp.where(seq == s, read[s * values : (s + 1) * values], total)
        ro[part, half] = total
        shared = vts[part, half]
        zero = jnp.zeros_like(shared)
        left = jnp.concatenate([jnp.where(seq == s, shared, zero) for s in range(block)], axis=0)
        update = nn(left, kps[h, half, :])
        for s in range(block):
            nm_ref[s, h] = (
                dfull[h, pl.ds(first + s, 1), :] * memory[s]
                + update[s * values : (s + 1) * values]
            )

    @pl.when(step == steps - 1)
    def _():
        same = iota((rows, rows), 0) // span == iota((rows, rows), 1) // span
        spread = iota((seqs, rows), 0) == iota((seqs, rows), 1) // span
        eye = iota((values, values), 0) == iota((values, values), 1)
        q = q_ref[...]
        owner = iota(q.shape, 0) // keys

        z = lax.axis_index("kv")
        gains = gain_ref[:, :values]
        for i in range(1, gain_ref.shape[1] // values):
            gains = jnp.where(
                lax.axis_index("tp") == i, gain_ref[:, i * values : (i + 1) * values], gains
            )
        local = gains[:heads]
        for i in range(1, gain_ref.shape[0] // heads):
            local = jnp.where(z == i, gains[i * heads : (i + 1) * heads], local)

        def tile(w):
            w = jnp.concatenate([w] * (8 // span), axis=0)
            return jnp.broadcast_to(w[None], (rows // 8, 8, rows)).reshape(rows, rows)

        for h in range(heads):
            part = slice(h * values, (h + 1) * values)
            only = jnp.where(owner == h, q, jnp.zeros_like(q))
            w = wexp[h]
            w_prev = jnp.where(same, tile(w[:span]) * nn(pk_ref[...], only), 0.0)
            w_new = jnp.where(same, tile(w[span : 2 * span]) * nn(k_ref[...], only), 0.0)
            carry = w[2 * span : 2 * span + 1]
            floor = w[2 * span + 1 : 2 * span + 2]
            top = nn(pv_ref[part, :], w_prev.astype(BF16)) + nn(v_ref[part, :], w_new.astype(BF16))
            top = top + carry * ro[part, :]
            nq = nn(nrm_ref[:, h, :].astype(BF16), q_ref[h * keys : (h + 1) * keys, :])
            nq = jnp.sum(jnp.where(spread, nq, 0.0), axis=0, keepdims=True)
            under = jnp.sum(w_prev + w_new, axis=0, keepdims=True) + carry * nq
            cell = top / jnp.maximum(jnp.abs(under), floor)
            sq_ref[h : h + 1, :] = jnp.sum(cell * cell, axis=0, keepdims=True)
            gain = nn(
                jnp.where(eye, local[h : h + 1, :], 0.0), jnp.ones((values, rows), F32), HIGHEST
            )
            g_ref[part, :] = (jax.nn.sigmoid(og_ref[part, :]) * cell * gain).astype(BF16)


def output_kernel(
    n, full_values, halves,
    g_ref, sq_ref, w_ref,
    y_ref,
    g_in, sq_in, both, from_low, from_high, to_high, to_low, total,
    side_send, side_recv, up_send, up_recv, down_send, down_recv,
):
    z = lax.axis_index("kv")
    c = lax.axis_index("tp")
    enter(n, z, c)
    side = {"tp": 1 - c}
    swaps = [
        pltpu.make_async_remote_copy(
            src_ref=src, dst_ref=dst, send_sem=side_send.at[i], recv_sem=side_recv.at[i],
            device_id=side, device_id_type=MESH,
        )
        for i, (src, dst) in enumerate(((g_ref, g_in), (sq_ref, sq_in)))
    ]
    for swap in swaps:
        swap.start()
    for swap in swaps:
        swap.wait_recv()
    inv = lax.rsqrt((sq_ref[...] + sq_in[...]) / full_values + EPS)
    channels = g_ref.shape[0]
    heads = sq_ref.shape[0]
    values = channels // heads
    for i, src in enumerate((g_ref, g_in)):
        scaled = jnp.concatenate(
            [
                src[h * values : (h + 1) * values, :].astype(F32) * inv[h : h + 1, :]
                for h in range(heads)
            ],
            axis=0,
        )
        both[:, i * channels : (i + 1) * channels] = scaled.T.astype(BF16)

    height = both.shape[0] // halves

    def partial(d, half):
        return nn(both[half * height : (half + 1) * height], w_ref[d])

    def upward(d, half):
        return pltpu.make_async_remote_copy(
            src_ref=to_high.at[d, half], dst_ref=from_low.at[d, half],
            send_sem=up_send.at[d, half], recv_sem=up_recv.at[d, half],
            device_id={"kv": z + 1}, device_id_type=MESH,
        )

    def downward(d, half):
        return pltpu.make_async_remote_copy(
            src_ref=to_low.at[d, half], dst_ref=from_high.at[d, half],
            send_sem=down_send.at[d, half], recv_sem=down_recv.at[d, half],
            device_id={"kv": z - 1}, device_id_type=MESH,
        )

    def step(i, carry):
        high = n - 1 - i + z
        low = i - (n - 1 - z)
        for half in range(halves):
            @pl.when((high > z) & (high <= n - 1))
            def _():
                term = partial(high, half)

                @pl.when(z == 0)
                def _():
                    to_high[high, half] = term.astype(BF16)

                @pl.when(z > 0)
                def _():
                    upward(high, half).wait_recv()
                    to_high[high, half] = (term + from_low[high, half].astype(F32)).astype(BF16)

                upward(high, half).start()

            @pl.when((low < z) & (low >= 0))
            def _():
                term = partial(low, half)

                @pl.when(z == n - 1)
                def _():
                    to_low[low, half] = term.astype(BF16)

                @pl.when(z < n - 1)
                def _():
                    downward(low, half).wait_recv()
                    to_low[low, half] = (term + from_high[low, half].astype(F32)).astype(BF16)

                downward(low, half).start()

        return carry

    lax.fori_loop(0, 2 * n - 2, step, 0)
    for half in range(halves):
        total[half] = partial(z, half)
    for half in range(halves):
        @pl.when(z > 0)
        def _():
            upward(z, half).wait_recv()
            total[half] += from_low[z, half].astype(F32)

        @pl.when(z < n - 1)
        def _():
            downward(z, half).wait_recv()
            total[half] += from_high[z, half].astype(F32)

    seqs, span, width = y_ref.shape
    y_ref[...] = total[...].reshape(seqs, span, width).astype(BF16)

    def drain(i, carry):
        for half in range(halves):
            @pl.when(i > z)
            def _():
                upward(i, half).wait_send()

            @pl.when(i < z)
            def _():
                downward(i, half).wait_send()

        return carry

    lax.fori_loop(0, n, drain, 0)
    for swap in swaps:
        swap.wait_send()


def shards(
    n, tokens, norm_gain, w_query, w_key, w_value, w_outgate, w_input, w_forget, forget_bias,
    head_gain, w_out, memory, normalizer, stabilizer, prev_keys, prev_values, prev_input,
    prev_forget, accepted,
):
    seqs, span, width = tokens.shape
    depth, heads, keys = w_query.shape
    values = w_value.shape[2]
    rows = seqs * span
    hk, hv = heads * keys, heads * values
    all_heads = w_input.shape[1]
    sds = jax.ShapeDtypeStruct
    vm = pl.BlockSpec(memory_space=pltpu.VMEM)
    hbm = pl.BlockSpec(memory_space=pl.ANY)
    flip = lambda w: w.transpose(1, 2, 0).reshape(-1, depth)

    halves = 2
    height = rows // halves
    channels = 2 * hk + 2 * hv + 2 * all_heads
    q, k, v, og, gi, gf, wout = pl.pallas_call(
        functools.partial(project_kernel, n, keys, halves),
        out_shape=[
            sds((hk, rows), BF16), sds((rows, hk), BF16), sds((hv, rows), BF16),
            sds((hv, rows), F32), sds((heads, rows), F32), sds((heads, rows), F32),
            sds((n, 2 * hv, width), BF16),
        ],
        in_specs=[vm, vm] + [hbm] * 6 + [vm, hbm],
        out_specs=[vm] * 7,
        scratch_shapes=[
            pltpu.VMEM((2 * n, halves, height, width), BF16),
            pltpu.VMEM((channels, depth), BF16),
            pltpu.VMEM((channels, rows), F32),
            pltpu.VMEM((rows, 128), F32),
            pltpu.SemaphoreType.DMA((6,)),
            pltpu.SemaphoreType.DMA((n,)),
            pltpu.SemaphoreType.DMA((3, 2 * n, halves)),
            pltpu.SemaphoreType.DMA((2 * n, halves)),
            pltpu.SemaphoreType.DMA((n,)),
            pltpu.SemaphoreType.DMA((n,)),
        ],
        compiler_params=pltpu.CompilerParams(
            collective_id=0, has_side_effects=True, vmem_limit_bytes=VMEM_LIMIT
        ),
        name="project",
    )(
        tokens, norm_gain.reshape(1, depth),
        flip(w_query), flip(w_key), flip(w_value), flip(w_outgate),
        w_input.T, w_forget.T, forget_bias.reshape(1, all_heads), w_out.reshape(hv, -1),
    )

    block = 8
    whole = lambda *shape: pl.BlockSpec(shape, lambda i: (0,) * len(shape))
    tile = pl.BlockSpec((block, heads, values, keys), lambda i: (i, 0, 0, 0))
    new_memory, new_normalizer, ns, ni, nf, g, sq = pl.pallas_call(
        recurrent_kernel,
        grid=(seqs // block,),
        out_shape=[
            sds(memory.shape, F32), sds(normalizer.shape, F32), sds((heads, seqs), F32),
            sds((span, heads, seqs), F32), sds((span, heads, seqs), F32),
            sds((hv, rows), BF16), sds((heads, rows), F32),
        ],
        in_specs=[
            whole(hk, rows), whole(rows, hk), whole(hv, rows), whole(hv, rows),
            whole(heads, rows), whole(heads, rows), whole(rows, hk), whole(hv, rows),
            whole(span, heads, seqs), whole(span, heads, seqs), whole(1, seqs),
            whole(heads, seqs), whole(seqs, heads, keys), whole(*head_gain.shape), tile,
        ],
        out_specs=[
            tile, whole(seqs, heads, keys), whole(heads, seqs), whole(span, heads, seqs),
            whole(span, heads, seqs), whole(hv, rows), whole(heads, rows),
        ],
        scratch_shapes=[
            pltpu.VMEM((hv, rows), BF16), pltpu.VMEM((heads, rows, keys), BF16),
            pltpu.VMEM((heads, seqs, keys), F32), pltpu.VMEM((heads, 16, rows), F32),
            pltpu.VMEM((hv, rows), F32),
        ],
        compiler_params=pltpu.CompilerParams(vmem_limit_bytes=VMEM_LIMIT),
        name="recurrent",
    )(
        q, k, v, og, gi, gf, prev_keys.reshape(rows, hk),
        prev_values.reshape(rows, hv).T,
        prev_input.transpose(1, 2, 0), prev_forget.transpose(1, 2, 0),
        accepted.reshape(1, seqs), stabilizer.T, normalizer, head_gain, memory,
    )

    y = pl.pallas_call(
        functools.partial(output_kernel, n, values * 2, halves),
        out_shape=sds(tokens.shape, BF16),
        in_specs=[vm] * 3,
        out_specs=vm,
        scratch_shapes=[pltpu.VMEM((hv, rows), BF16), pltpu.VMEM((heads, rows), F32)]
        + [pltpu.VMEM((rows, 2 * hv), BF16)]
        + [pltpu.VMEM((n, halves, height, width), BF16)] * 4
        + [pltpu.VMEM((halves, height, width), F32)]
        + [pltpu.SemaphoreType.DMA((2,))] * 2
        + [pltpu.SemaphoreType.DMA((n, halves))] * 4,
        compiler_params=pltpu.CompilerParams(
            collective_id=1, has_side_effects=True, vmem_limit_bytes=VMEM_LIMIT
        ),
        name="output",
    )(g, sq, wout)

    return (
        y,
        new_memory,
        new_normalizer,
        ns.T,
        k.reshape(seqs, span, heads, keys),
        v.T.reshape(seqs, span, heads, values),
        ni.transpose(2, 0, 1),
        nf.transpose(2, 0, 1),
    )


def solution(mesh):
    return jax.shard_map(
        functools.partial(shards, mesh.shape["kv"]),
        mesh=mesh,
        in_specs=(
            P(("grp", "dp"), None, ("kv", "tp")),
            P(),
            P(None, "kv", None),
            P(None, "kv", None),
            P(None, "kv", "tp"),
            P(None, "kv", "tp"),
            P(),
            P(),
            P(),
            P(),
            P("kv", "tp", None),
            P(("grp", "dp"), "kv", "tp", None),
            P(("grp", "dp"), "kv", None),
            P(("grp", "dp"), "kv"),
            P(("grp", "dp"), None, "kv", None),
            P(("grp", "dp"), None, "kv", "tp"),
            P(("grp", "dp"), None, "kv"),
            P(("grp", "dp"), None, "kv"),
            P(("grp", "dp")),
        ),
        out_specs=(
            P(("grp", "dp"), None, ("kv", "tp")),
            P(("grp", "dp"), "kv", "tp", None),
            P(("grp", "dp"), "kv", None),
            P(("grp", "dp"), "kv"),
            P(("grp", "dp"), None, "kv", None),
            P(("grp", "dp"), None, "kv", "tp"),
            P(("grp", "dp"), None, "kv"),
            P(("grp", "dp"), None, "kv"),
        ),
        check_vma=False,
    )
```

```python
import functools
import jax
import jax.numpy as jnp
from jax import lax
from jax.sharding import PartitionSpec as P
from jax.experimental import pallas as pl
from jax.experimental.pallas import tpu as pltpu

EPS = 1e-06
FAR_NEGATIVE = -1e30
HIGHEST = lax.Precision.HIGHEST
MESH = pl.DeviceIdType.MESH
F32 = jnp.float32
BF16 = jnp.bfloat16
VMEM_LIMIT = 60 << 20


def nn(a, b, precision=None):
    return lax.dot_general(
        a, b, (((1,), (0,)), ((), ())), precision=precision, preferred_element_type=F32
    )


def nt(a, b, precision=None):
    return lax.dot_general(
        a, b, (((1,), (1,)), ((), ())), precision=precision, preferred_element_type=F32
    )


def enter(n, z, c):
    barrier = pltpu.get_barrier_semaphore()
    pl.semaphore_signal(barrier, inc=1, device_id={"tp": 1 - c}, device_id_type=MESH)

    @pl.when(z > 0)
    def _():
        pl.semaphore_signal(barrier, inc=1, device_id={"kv": z - 1}, device_id_type=MESH)

    @pl.when(z < n - 1)
    def _():
        pl.semaphore_signal(barrier, inc=1, device_id={"kv": z + 1}, device_id_type=MESH)

    peers = 1 + (z > 0).astype(jnp.int32) + (z < n - 1).astype(jnp.int32)
    pl.semaphore_wait(barrier, peers)


def project_kernel(
    n, key_size, halves,
    x_ref, gain_ref, wq_hbm, wk_hbm, wv_hbm, wo_hbm, wi_hbm, wf_hbm, bias_ref, pk_ref, pv_ref, out_hbm,
    q_out, k_out, v_out, og_out, gi_out, gf_out, pk_out, pv_out, wout_out,
    xg, weights, acc, squares,
    load_sem, send_sem, recv_sem, wsend_sem, wrecv_sem,
):
    z = lax.axis_index("kv")
    c = lax.axis_index("tp")
    width = x_ref.shape[2]
    rows = x_ref.shape[0] * x_ref.shape[1]
    height = rows // halves
    loads, spans, at = [], [], 0
    for i, src in enumerate((wq_hbm, wk_hbm, wv_hbm, wo_hbm, wi_hbm, wf_hbm)):
        size = src.shape[0]
        spans.append(slice(at, at + size))
        loads.append(
            pltpu.make_async_copy(src, weights.at[pl.ds(at, size)], load_sem.at[i])
        )
        at += size
    for load in loads:
        load.start()
    mine = 2 * z + c
    flat = x_ref[...].reshape(rows, width)
    for half in range(halves):
        xg[mine, half] = flat[half * height : (half + 1) * height]
    acc[...] = jnp.zeros_like(acc)
    squares[...] = jnp.zeros_like(squares)
    enter(n, z, c)

    def hop(slot, half, way, target):
        return pltpu.make_async_remote_copy(
            src_ref=xg.at[slot, half], dst_ref=xg.at[slot, half],
            send_sem=send_sem.at[way, slot, half], recv_sem=recv_sem.at[slot, half],
            device_id=target, device_id_type=MESH,
        )

    up, down, side = {"kv": z + 1}, {"kv": z - 1}, {"tp": 1 - c}

    for half in range(halves):
        @pl.when(z < n - 1)
        def _():
            hop(mine, half, 0, up).start()

        @pl.when(z > 0)
        def _():
            hop(mine, half, 1, down).start()

        hop(mine, half, 2, side).start()


    def out_piece(i):
        col = pl.multiple_of((2 * i + 1 - c) * width, width)
        return pltpu.make_async_remote_copy(
            src_ref=out_hbm.at[:, pl.ds(col, width)],
            dst_ref=wout_out.at[i],
            send_sem=wsend_sem.at[i], recv_sem=wrecv_sem.at[i],
            device_id=side, device_id_type=MESH,
        )

    for i in range(n):
        out_piece(i).start()
    heads, values = pv_ref.shape[2:]
    old_keys = pk_ref[...].astype(F32).reshape(rows, heads, key_size)
    old_values = pv_ref[...].astype(F32).reshape(rows, heads, values)
    for h in range(heads):
        pk_out[:, h * key_size : (h + 1) * key_size] = old_keys[:, h, :].astype(BF16)
        pv_out[h * values : (h + 1) * values, :] = old_values[:, h, :].T.astype(BF16)
    for load in loads:
        load.wait()

    def process(slot):
        cols = pl.ds(pl.multiple_of(slot * width, width), width)
        x = jnp.concatenate([xg[slot, half] for half in range(halves)], axis=0).astype(F32)
        square = x * x
        total = squares[...]
        for i in range(width // 128):
            total = total + square[:, i * 128 : (i + 1) * 128]
        squares[...] = total
        acc[...] += nt(weights[:, cols], (x * gain_ref[:, cols]).astype(BF16))

    def process_owner(owner):
        process(2 * owner + c)
        slot = 2 * owner + 1 - c
        for half in range(halves):
            hop(slot, half, 2, side).wait_recv()
        process(slot)

    def forward(k, half):
        @pl.when(z - k >= 0)
        def _():
            slot = 2 * (z - k) + c
            hop(slot, half, 0, up).wait_recv()

            @pl.when(z < n - 1)
            def _():
                hop(slot, half, 0, up).start()

            hop(slot, half, 2, side).start()

        @pl.when(z + k <= n - 1)
        def _():
            slot = 2 * (z + k) + c
            hop(slot, half, 1, down).wait_recv()

            @pl.when(z > 0)
            def _():
                hop(slot, half, 1, down).start()

            hop(slot, half, 2, side).start()

    def step(k, carry):
        for half in range(halves - 1):
            forward(k, half)

        @pl.when(z - (k - 1) >= 0)
        def _():
            process_owner(z - (k - 1))

        forward(k, halves - 1)

        @pl.when((z + k - 1 <= n - 1) & (k > 1))
        def _():
            process_owner(z + k - 1)

        return carry

    lax.fori_loop(1, n + 1, step, 0)

    depth = gain_ref.shape[1]
    total = nt(jnp.ones((8, 128), F32), squares[...], HIGHEST)
    inv = lax.rsqrt(total[0:1] / depth + EPS)
    q, k, v, og, gi, gf = [acc[part, :] * inv for part in spans]
    q_out[...] = (q.astype(BF16).astype(F32) * key_size ** (-0.5)).astype(BF16)
    k_out[...] = k.T.astype(BF16)
    v_out[...] = v.astype(BF16)
    og_out[...] = og
    all_heads = gf.shape[0]
    diagonal = lax.broadcasted_iota(jnp.int32, (all_heads, all_heads), 0) == (
        lax.broadcasted_iota(jnp.int32, (all_heads, all_heads), 1)
    )
    shift = nn(jnp.where(diagonal, bias_ref[...], 0.0), jnp.ones(gf.shape, F32), HIGHEST)
    raw = gf + shift
    gf = jnp.minimum(raw, 0.0) - jnp.log1p(jnp.exp(-jnp.abs(raw)))
    local_heads = gi_out.shape[0]
    for values, out in ((gi, gi_out), (gf, gf_out)):
        total = values[:local_heads]
        for i in range(1, n):
            total = jnp.where(z == i, values[i * local_heads : (i + 1) * local_heads], total)
        out[...] = total

    for i in range(n):
        out_piece(i).wait()

    def drain(i, carry):
        slot = 2 * i + c
        for half in range(halves):
            @pl.when((i <= z) & (z < n - 1))
            def _():
                hop(slot, half, 0, up).wait_send()

            @pl.when((i >= z) & (z > 0))
            def _():
                hop(slot, half, 1, down).wait_send()

            hop(slot, half, 2, side).wait_send()
        return carry

    lax.fori_loop(0, n, drain, 0)


def recurrent_kernel(
    q_ref, k_ref, v_ref, og_ref, gi_ref, gf_ref, pk_ref, pv_ref, pi_ref, pf_ref,
    acc_ref, stab_ref, nrm_ref, gain_ref, mem_ref,
    nm_ref, nn_ref, ns_ref, ni_ref, nf_ref, g_ref, sq_ref,
    vts, kps, dfull, wexp, ro,
):
    step = pl.program_id(0)
    steps = pl.num_programs(0)
    block, heads, values, keys = mem_ref.shape
    span, _, seqs = pi_ref.shape
    rows = seqs * span
    lanes = 128
    iota = lambda shape, d: lax.broadcasted_iota(jnp.int32, shape, d)

    @pl.when(step == 0)
    def _():
        spread = (iota((seqs, rows), 0) == iota((seqs, rows), 1) // span)
        expand = spread.astype(F32)
        lane_pos = iota((span, rows), 1) % span == iota((span, rows), 0)
        dropped = iota((span, seqs), 0) >= acc_ref[...]
        ro[...] = jnp.zeros_like(ro)
        single = [
            jnp.where(lane_pos, ref[h : h + 1, :], 0.0)
            for h in range(heads)
            for ref in (gi_ref, gf_ref)
        ]
        compact = nt(jnp.concatenate(single, axis=0), expand, HIGHEST)
        position = iota((2 * span, seqs), 0)
        stack, decays = [], []
        for h in range(heads):
            stab = stab_ref[h : h + 1, :]
            f = jnp.where(dropped, 0.0, pf_ref[:, h, :])
            i = jnp.where(dropped, FAR_NEGATIVE, pi_ref[:, h, :])
            new_i = compact[2 * h * span : (2 * h + 1) * span]
            new_f = compact[(2 * h + 1) * span : (2 * h + 2) * span]
            ni_ref[:, h, :] = new_i
            nf_ref[:, h, :] = new_f
            total = []
            for j in range(span):
                total.append(f[j : j + 1] + total[-1] if total else f[0:1])
            e = total[-1]
            for j in range(span):
                total.append(total[-1] + new_f[j : j + 1])
            run_prev = jnp.concatenate(total[:span], axis=0)
            run_all = jnp.concatenate(total, axis=0)
            in_all = jnp.concatenate([i, new_i], axis=0)
            u = e - run_prev + i
            ns = jnp.maximum(e + stab, jnp.max(u, axis=0, keepdims=True))
            ns_ref[h : h + 1, :] = ns
            decays.append(jnp.exp(e + stab - ns))
            stack += [jnp.exp(u - ns), jnp.zeros((8 - span, seqs), F32)]
            for t in range(span):
                latest = total[span + t]
                d = jnp.where(position <= span + t, latest - run_all + in_all, FAR_NEGATIVE)
                g = latest + stab
                top = jnp.maximum(jnp.max(d, axis=0, keepdims=True), g)
                pad = jnp.zeros((16 - 2 * span - 2, seqs), F32)
                stack += [jnp.exp(d - top), jnp.exp(g - top), jnp.exp(-top), pad]
        wide = nn(jnp.concatenate(stack, axis=0), expand, HIGHEST)
        decays = jnp.concatenate(decays + [jnp.zeros((8 - heads, seqs), F32)], axis=0).T
        each = 8 + 16 * span
        for h in range(heads):
            base = h * each
            share_row = jnp.sum(
                jnp.where(lane_pos, wide[base : base + span], 0.0), axis=0, keepdims=True
            )
            kps[h] = pk_ref[:, h * keys : (h + 1) * keys]
            part = slice(h * values, (h + 1) * values)
            vts[part, :] = (pv_ref[part, :].astype(F32) * share_row).astype(BF16)
            full = jnp.broadcast_to(decays[:, h : h + 1], (seqs, keys))
            dfull[h] = full
            mixed = jnp.where(spread, share_row, 0.0).astype(BF16)
            nn_ref[:, h, :] = full * nrm_ref[:, h, :] + nn(mixed, kps[h])
            gathered = jnp.zeros((16, rows), F32)
            for t in range(span):
                at = base + 8 + 16 * t
                gathered = jnp.where(
                    iota((16, rows), 1) % span == t, wide[at : at + 16], gathered
                )
            wexp[h] = gathered

    first = step * block
    start = pl.multiple_of((first * span) // lanes * lanes, lanes)
    half = pl.ds(start, lanes)
    seq = (iota((values, lanes), 1) + start) // span - first
    for h in range(heads):
        part = slice(h * values, (h + 1) * values)
        memory = [mem_ref[s, h] for s in range(block)]
        packed = jnp.concatenate([m.astype(BF16) for m in memory], axis=0)
        read = nn(packed, q_ref[h * keys : (h + 1) * keys, half])
        total = ro[part, half]
        for s in range(block):
            total = jnp.where(seq == s, read[s * values : (s + 1) * values], total)
        ro[part, half] = total
        shared = vts[part, half]
        zero = jnp.zeros_like(shared)
        left = jnp.concatenate([jnp.where(seq == s, shared, zero) for s in range(block)], axis=0)
        update = nn(left, kps[h, half, :])
        for s in range(block):
            nm_ref[s, h] = (
                dfull[h, pl.ds(first + s, 1), :] * memory[s]
                + update[s * values : (s + 1) * values]
            )

    @pl.when(step == steps - 1)
    def _():
        same = iota((rows, rows), 0) // span == iota((rows, rows), 1) // span
        spread = iota((seqs, rows), 0) == iota((seqs, rows), 1) // span
        q = q_ref[...]
        owner = iota(q.shape, 0) // keys

        z = lax.axis_index("kv")
        gains = gain_ref[:, :values]
        for i in range(1, gain_ref.shape[1] // values):
            gains = jnp.where(
                lax.axis_index("tp") == i, gain_ref[:, i * values : (i + 1) * values], gains
            )
        local = gains[:heads]
        for i in range(1, gain_ref.shape[0] // heads):
            local = jnp.where(z == i, gains[i * heads : (i + 1) * heads], local)

        columns = jnp.concatenate([local, jnp.zeros((8 - heads, values), F32)], axis=0).T

        def tile(w):
            w = jnp.concatenate([w] * (8 // span), axis=0)
            return jnp.broadcast_to(w[None], (rows // 8, 8, rows)).reshape(rows, rows)

        for h in range(heads):
            part = slice(h * values, (h + 1) * values)
            only = jnp.where(owner == h, q, jnp.zeros_like(q))
            w = wexp[h]
            w_prev = jnp.where(same, tile(w[:span]) * nn(pk_ref[...], only), 0.0)
            w_new = jnp.where(same, tile(w[span : 2 * span]) * nn(k_ref[...], only), 0.0)
            carry = w[2 * span : 2 * span + 1]
            floor = w[2 * span + 1 : 2 * span + 2]
            top = nn(pv_ref[part, :], w_prev.astype(BF16)) + nn(v_ref[part, :], w_new.astype(BF16))
            top = top + carry * ro[part, :]
            nq = nn(nrm_ref[:, h, :].astype(BF16), q_ref[h * keys : (h + 1) * keys, :])
            nq = jnp.sum(jnp.where(spread, nq, 0.0), axis=0, keepdims=True)
            under = jnp.sum(w_prev + w_new, axis=0, keepdims=True) + carry * nq
            cell = top / jnp.maximum(jnp.abs(under), floor)
            sq_ref[h : h + 1, :] = jnp.sum(cell * cell, axis=0, keepdims=True)
            gain = columns[:, h : h + 1]
            g_ref[part, :] = (jax.nn.sigmoid(og_ref[part, :]) * cell * gain).astype(BF16)


def output_kernel(
    n, full_values, halves,
    g_ref, sq_ref, own_hbm, other_hbm,
    y_ref,
    g_in, sq_in, both, from_low, from_high, to_high, to_low, total, w_ref,
    load_sem,
    side_send, side_recv, up_send, up_recv, down_send, down_recv,
):
    z = lax.axis_index("kv")
    c = lax.axis_index("tp")
    channels = g_ref.shape[0]
    width = y_ref.shape[2]
    loads = []
    for d in range(n):
        col = pl.multiple_of((2 * d + c) * width, width)
        loads += [
            pltpu.make_async_copy(
                own_hbm.at[:, pl.ds(col, width)], w_ref.at[d, pl.ds(0, channels)],
                load_sem.at[2 * d],
            ),
            pltpu.make_async_copy(
                other_hbm.at[d], w_ref.at[d, pl.ds(channels, channels)], load_sem.at[2 * d + 1]
            ),
        ]
    for load in loads:
        load.start()
    enter(n, z, c)
    side = {"tp": 1 - c}
    swaps = [
        pltpu.make_async_remote_copy(
            src_ref=src, dst_ref=dst, send_sem=side_send.at[i], recv_sem=side_recv.at[i],
            device_id=side, device_id_type=MESH,
        )
        for i, (src, dst) in enumerate(((g_ref, g_in), (sq_ref, sq_in)))
    ]
    for swap in swaps:
        swap.start()
    for swap in swaps:
        swap.wait_recv()
    inv = lax.rsqrt((sq_ref[...] + sq_in[...]) / full_values + EPS)
    heads = sq_ref.shape[0]
    values = channels // heads
    for i, src in enumerate((g_ref, g_in)):
        scaled = jnp.concatenate(
            [
                src[h * values : (h + 1) * values, :].astype(F32) * inv[h : h + 1, :]
                for h in range(heads)
            ],
            axis=0,
        )
        both[:, i * channels : (i + 1) * channels] = scaled.T.astype(BF16)

    for load in loads:
        load.wait()
    height = both.shape[0] // halves

    def partial(d, half):
        return nn(both[half * height : (half + 1) * height], w_ref[d])

    def upward(d, half):
        return pltpu.make_async_remote_copy(
            src_ref=to_high.at[d, half], dst_ref=from_low.at[d, half],
            send_sem=up_send.at[d, half], recv_sem=up_recv.at[d, half],
            device_id={"kv": z + 1}, device_id_type=MESH,
        )

    def downward(d, half):
        return pltpu.make_async_remote_copy(
            src_ref=to_low.at[d, half], dst_ref=from_high.at[d, half],
            send_sem=down_send.at[d, half], recv_sem=down_recv.at[d, half],
            device_id={"kv": z - 1}, device_id_type=MESH,
        )

    def step(i, carry):
        high = n - 1 - i + z
        low = i - (n - 1 - z)
        for half in range(halves):
            @pl.when((high > z) & (high <= n - 1))
            def _():
                term = partial(high, half)

                @pl.when(z == 0)
                def _():
                    to_high[high, half] = term.astype(BF16)

                @pl.when(z > 0)
                def _():
                    upward(high, half).wait_recv()
                    to_high[high, half] = (term + from_low[high, half].astype(F32)).astype(BF16)

                upward(high, half).start()

            @pl.when((low < z) & (low >= 0))
            def _():
                term = partial(low, half)

                @pl.when(z == n - 1)
                def _():
                    to_low[low, half] = term.astype(BF16)

                @pl.when(z < n - 1)
                def _():
                    downward(low, half).wait_recv()
                    to_low[low, half] = (term + from_high[low, half].astype(F32)).astype(BF16)

                downward(low, half).start()

        return carry

    lax.fori_loop(0, 2 * n - 2, step, 0)
    for half in range(halves):
        total[half] = partial(z, half)
    for half in range(halves):
        @pl.when(z > 0)
        def _():
            upward(z, half).wait_recv()
            total[half] += from_low[z, half].astype(F32)

        @pl.when(z < n - 1)
        def _():
            downward(z, half).wait_recv()
            total[half] += from_high[z, half].astype(F32)

    seqs, span, width = y_ref.shape
    y_ref[...] = total[...].reshape(seqs, span, width).astype(BF16)

    def drain(i, carry):
        for half in range(halves):
            @pl.when(i > z)
            def _():
                upward(i, half).wait_send()

            @pl.when(i < z)
            def _():
                downward(i, half).wait_send()

        return carry

    lax.fori_loop(0, n, drain, 0)
    for swap in swaps:
        swap.wait_send()


def shards(
    n, tokens, norm_gain, w_query, w_key, w_value, w_outgate, w_input, w_forget, forget_bias,
    head_gain, w_out, memory, normalizer, stabilizer, prev_keys, prev_values, prev_input,
    prev_forget, accepted,
):
    seqs, span, width = tokens.shape
    depth, heads, keys = w_query.shape
    values = w_value.shape[2]
    rows = seqs * span
    hk, hv = heads * keys, heads * values
    all_heads = w_input.shape[1]
    sds = jax.ShapeDtypeStruct
    vm = pl.BlockSpec(memory_space=pltpu.VMEM)
    hbm = pl.BlockSpec(memory_space=pl.ANY)
    flip = lambda w: w.transpose(1, 2, 0).reshape(-1, depth)

    halves = 2
    height = rows // halves
    channels = 2 * hk + 2 * hv + 2 * all_heads
    q, k, v, og, gi, gf, pk, pv, wout = pl.pallas_call(
        functools.partial(project_kernel, n, keys, halves),
        out_shape=[
            sds((hk, rows), BF16), sds((rows, hk), BF16), sds((hv, rows), BF16),
            sds((hv, rows), F32), sds((heads, rows), F32), sds((heads, rows), F32),
            sds((rows, hk), BF16), sds((hv, rows), BF16), sds((n, hv, width), BF16),
        ],
        in_specs=[vm, vm] + [hbm] * 6 + [vm, vm, vm, hbm],
        out_specs=[vm] * 8 + [hbm],
        scratch_shapes=[
            pltpu.VMEM((2 * n, halves, height, width), BF16),
            pltpu.VMEM((channels, depth), BF16),
            pltpu.VMEM((channels, rows), F32),
            pltpu.VMEM((rows, 128), F32),
            pltpu.SemaphoreType.DMA((6,)),
            pltpu.SemaphoreType.DMA((3, 2 * n, halves)),
            pltpu.SemaphoreType.DMA((2 * n, halves)),
            pltpu.SemaphoreType.DMA((n,)),
            pltpu.SemaphoreType.DMA((n,)),
        ],
        compiler_params=pltpu.CompilerParams(
            collective_id=0, has_side_effects=True, vmem_limit_bytes=VMEM_LIMIT
        ),
        name="project",
    )(
        tokens, norm_gain.reshape(1, depth),
        flip(w_query), flip(w_key), flip(w_value), flip(w_outgate),
        w_input.T, w_forget.T, forget_bias.reshape(1, all_heads), prev_keys, prev_values,
        w_out.reshape(hv, -1),
    )

    block = 8
    whole = lambda *shape: pl.BlockSpec(shape, lambda i: (0,) * len(shape))
    tile = pl.BlockSpec((block, heads, values, keys), lambda i: (i, 0, 0, 0))
    new_memory, new_normalizer, ns, ni, nf, g, sq = pl.pallas_call(
        recurrent_kernel,
        grid=(seqs // block,),
        out_shape=[
            sds(memory.shape, F32), sds(normalizer.shape, F32), sds((heads, seqs), F32),
            sds((span, heads, seqs), F32), sds((span, heads, seqs), F32),
            sds((hv, rows), BF16), sds((heads, rows), F32),
        ],
        in_specs=[
            whole(hk, rows), whole(rows, hk), whole(hv, rows), whole(hv, rows),
            whole(heads, rows), whole(heads, rows), whole(rows, hk), whole(hv, rows),
            whole(span, heads, seqs), whole(span, heads, seqs), whole(1, seqs),
            whole(heads, seqs), whole(seqs, heads, keys), whole(*head_gain.shape), tile,
        ],
        out_specs=[
            tile, whole(seqs, heads, keys), whole(heads, seqs), whole(span, heads, seqs),
            whole(span, heads, seqs), whole(hv, rows), whole(heads, rows),
        ],
        scratch_shapes=[
            pltpu.VMEM((hv, rows), BF16), pltpu.VMEM((heads, rows, keys), BF16),
            pltpu.VMEM((heads, seqs, keys), F32), pltpu.VMEM((heads, 16, rows), F32),
            pltpu.VMEM((hv, rows), F32),
        ],
        compiler_params=pltpu.CompilerParams(vmem_limit_bytes=VMEM_LIMIT),
        name="recurrent",
    )(
        q, k, v, og, gi, gf, pk, pv,
        prev_input.transpose(1, 2, 0), prev_forget.transpose(1, 2, 0),
        accepted.reshape(1, seqs), stabilizer.T, normalizer, head_gain, memory,
    )

    y = pl.pallas_call(
        functools.partial(output_kernel, n, values * 2, halves),
        out_shape=sds(tokens.shape, BF16),
        in_specs=[vm, vm, hbm, hbm],
        out_specs=vm,
        scratch_shapes=[pltpu.VMEM((hv, rows), BF16), pltpu.VMEM((heads, rows), F32)]
        + [pltpu.VMEM((rows, 2 * hv), BF16)]
        + [pltpu.VMEM((n, halves, height, width), BF16)] * 4
        + [pltpu.VMEM((halves, height, width), F32), pltpu.VMEM((n, 2 * hv, width), BF16)]
        + [pltpu.SemaphoreType.DMA((2 * n,))]
        + [pltpu.SemaphoreType.DMA((2,))] * 2
        + [pltpu.SemaphoreType.DMA((n, halves))] * 4,
        compiler_params=pltpu.CompilerParams(
            collective_id=1, has_side_effects=True, vmem_limit_bytes=VMEM_LIMIT
        ),
        name="output",
    )(g, sq, w_out.reshape(hv, -1), wout)

    return (
        y,
        new_memory,
        new_normalizer,
        ns.T,
        k.reshape(seqs, span, heads, keys),
        v.T.reshape(seqs, span, heads, values),
        ni.transpose(2, 0, 1),
        nf.transpose(2, 0, 1),
    )


def solution(mesh):
    return jax.shard_map(
        functools.partial(shards, mesh.shape["kv"]),
        mesh=mesh,
        in_specs=(
            P(("grp", "dp"), None, ("kv", "tp")),
            P(),
            P(None, "kv", None),
            P(None, "kv", None),
            P(None, "kv", "tp"),
            P(None, "kv", "tp"),
            P(),
            P(),
            P(),
            P(),
            P("kv", "tp", None),
            P(("grp", "dp"), "kv", "tp", None),
            P(("grp", "dp"), "kv", None),
            P(("grp", "dp"), "kv"),
            P(("grp", "dp"), None, "kv", None),
            P(("grp", "dp"), None, "kv", "tp"),
            P(("grp", "dp"), None, "kv"),
            P(("grp", "dp"), None, "kv"),
            P(("grp", "dp")),
        ),
        out_specs=(
            P(("grp", "dp"), None, ("kv", "tp")),
            P(("grp", "dp"), "kv", "tp", None),
            P(("grp", "dp"), "kv", None),
            P(("grp", "dp"), "kv"),
            P(("grp", "dp"), None, "kv", None),
            P(("grp", "dp"), None, "kv", "tp"),
            P(("grp", "dp"), None, "kv"),
            P(("grp", "dp"), None, "kv"),
        ),
        check_vma=False,
    )
```

```python
import functools
import jax
import jax.numpy as jnp
from jax import lax
from jax.sharding import PartitionSpec as P
from jax.experimental import pallas as pl
from jax.experimental.pallas import tpu as pltpu

EPS = 1e-06
FAR_NEGATIVE = -1e30
HIGHEST = lax.Precision.HIGHEST
MESH = pl.DeviceIdType.MESH
F32 = jnp.float32
BF16 = jnp.bfloat16
VMEM_LIMIT = 60 << 20


def nn(a, b, precision=None):
    return lax.dot_general(
        a, b, (((1,), (0,)), ((), ())), precision=precision, preferred_element_type=F32
    )


def nt(a, b, precision=None):
    return lax.dot_general(
        a, b, (((1,), (1,)), ((), ())), precision=precision, preferred_element_type=F32
    )


def enter(n, z, c):
    barrier = pltpu.get_barrier_semaphore()
    pl.semaphore_signal(barrier, inc=1, device_id={"tp": 1 - c}, device_id_type=MESH)

    @pl.when(z > 0)
    def _():
        pl.semaphore_signal(barrier, inc=1, device_id={"kv": z - 1}, device_id_type=MESH)

    @pl.when(z < n - 1)
    def _():
        pl.semaphore_signal(barrier, inc=1, device_id={"kv": z + 1}, device_id_type=MESH)

    peers = 1 + (z > 0).astype(jnp.int32) + (z < n - 1).astype(jnp.int32)
    pl.semaphore_wait(barrier, peers)


def project_kernel(
    n, key_size, halves,
    x_ref, gain_ref, wq_hbm, wk_hbm, wv_hbm, wo_hbm, wi_hbm, wf_hbm, bias_ref, pk_ref, pv_ref, out_hbm,
    q_out, k_out, v_out, og_out, gi_out, gf_out, pk_out, pv_out, wout_out,
    xg, weights, acc, squares,
    load_sem, send_sem, recv_sem, wsend_sem, wrecv_sem,
):
    z = lax.axis_index("kv")
    c = lax.axis_index("tp")
    width = x_ref.shape[2]
    rows = x_ref.shape[0] * x_ref.shape[1]
    height = rows // halves
    loads, spans, at = [], [], 0
    for i, src in enumerate((wq_hbm, wk_hbm, wv_hbm, wo_hbm, wi_hbm, wf_hbm)):
        size = src.shape[0]
        spans.append(slice(at, at + size))
        loads.append(
            pltpu.make_async_copy(src, weights.at[pl.ds(at, size)], load_sem.at[i])
        )
        at += size
    for load in loads:
        load.start()
    mine = 2 * z + c
    flat = x_ref[...].reshape(rows, width)
    for half in range(halves):
        xg[mine, half] = flat[half * height : (half + 1) * height]
    acc[...] = jnp.zeros_like(acc)
    squares[...] = jnp.zeros_like(squares)
    enter(n, z, c)

    def hop(slot, half, way, target):
        return pltpu.make_async_remote_copy(
            src_ref=xg.at[slot, half], dst_ref=xg.at[slot, half],
            send_sem=send_sem.at[way, slot, half], recv_sem=recv_sem.at[slot, half],
            device_id=target, device_id_type=MESH,
        )

    up, down, side = {"kv": z + 1}, {"kv": z - 1}, {"tp": 1 - c}

    for half in range(halves):
        @pl.when(z < n - 1)
        def _():
            hop(mine, half, 0, up).start()

        @pl.when(z > 0)
        def _():
            hop(mine, half, 1, down).start()

        hop(mine, half, 2, side).start()


    def out_piece(i):
        col = pl.multiple_of((2 * i + 1 - c) * width, width)
        return pltpu.make_async_remote_copy(
            src_ref=out_hbm.at[:, pl.ds(col, width)],
            dst_ref=wout_out.at[i],
            send_sem=wsend_sem.at[i], recv_sem=wrecv_sem.at[i],
            device_id=side, device_id_type=MESH,
        )

    for i in range(n):
        out_piece(i).start()
    heads, values = pv_ref.shape[2:]
    old_keys = pk_ref[...].astype(F32).reshape(rows, heads, key_size)
    old_values = pv_ref[...].astype(F32).reshape(rows, heads, values)
    for h in range(heads):
        pk_out[:, h * key_size : (h + 1) * key_size] = old_keys[:, h, :].astype(BF16)
        pv_out[h * values : (h + 1) * values, :] = old_values[:, h, :].T.astype(BF16)
    for load in loads:
        load.wait()

    def process(slot):
        cols = pl.ds(pl.multiple_of(slot * width, width), width)
        x = jnp.concatenate([xg[slot, half] for half in range(halves)], axis=0).astype(F32)
        square = x * x
        total = squares[...]
        for i in range(width // 128):
            total = total + square[:, i * 128 : (i + 1) * 128]
        squares[...] = total
        acc[...] += nt(weights[:, cols], (x * gain_ref[:, cols]).astype(BF16))

    def process_owner(owner):
        process(2 * owner + c)
        slot = 2 * owner + 1 - c
        for half in range(halves):
            hop(slot, half, 2, side).wait_recv()
        process(slot)

    def forward(k, half):
        @pl.when(z - k >= 0)
        def _():
            slot = 2 * (z - k) + c
            hop(slot, half, 0, up).wait_recv()

            @pl.when(z < n - 1)
            def _():
                hop(slot, half, 0, up).start()

            hop(slot, half, 2, side).start()

        @pl.when(z + k <= n - 1)
        def _():
            slot = 2 * (z + k) + c
            hop(slot, half, 1, down).wait_recv()

            @pl.when(z > 0)
            def _():
                hop(slot, half, 1, down).start()

            hop(slot, half, 2, side).start()

    def step(k, carry):
        for half in range(halves - 1):
            forward(k, half)

        @pl.when(z - (k - 1) >= 0)
        def _():
            process_owner(z - (k - 1))

        forward(k, halves - 1)

        @pl.when((z + k - 1 <= n - 1) & (k > 1))
        def _():
            process_owner(z + k - 1)

        return carry

    lax.fori_loop(1, n + 1, step, 0)

    depth = gain_ref.shape[1]
    total = nt(jnp.ones((8, 128), F32), squares[...], HIGHEST)
    inv = lax.rsqrt(total[0:1] / depth + EPS)
    q, k, v, og, gi, gf = [acc[part, :] * inv for part in spans]
    q_out[...] = (q.astype(BF16).astype(F32) * key_size ** (-0.5)).astype(BF16)
    k_out[...] = k.T.astype(BF16)
    v_out[...] = v.astype(BF16)
    og_out[...] = og
    all_heads = gf.shape[0]
    diagonal = lax.broadcasted_iota(jnp.int32, (all_heads, all_heads), 0) == (
        lax.broadcasted_iota(jnp.int32, (all_heads, all_heads), 1)
    )
    shift = nn(jnp.where(diagonal, bias_ref[...], 0.0), jnp.ones(gf.shape, F32), HIGHEST)
    raw = gf + shift
    gf = jnp.minimum(raw, 0.0) - jnp.log1p(jnp.exp(-jnp.abs(raw)))
    local_heads = gi_out.shape[0]
    for values, out in ((gi, gi_out), (gf, gf_out)):
        total = values[:local_heads]
        for i in range(1, n):
            total = jnp.where(z == i, values[i * local_heads : (i + 1) * local_heads], total)
        out[...] = total

    for i in range(n):
        out_piece(i).wait()

    def drain(i, carry):
        slot = 2 * i + c
        for half in range(halves):
            @pl.when((i <= z) & (z < n - 1))
            def _():
                hop(slot, half, 0, up).wait_send()

            @pl.when((i >= z) & (z > 0))
            def _():
                hop(slot, half, 1, down).wait_send()

            hop(slot, half, 2, side).wait_send()
        return carry

    lax.fori_loop(0, n, drain, 0)


def recurrent_kernel(
    q_ref, k_ref, v_ref, og_ref, gi_ref, gf_ref, pk_ref, pv_ref, pi_ref, pf_ref,
    acc_ref, stab_ref, nrm_ref, gain_ref, mem_ref,
    nm_ref, nn_ref, ns_ref, ni_ref, nf_ref, g_ref, sq_ref,
    vts, kps, dfull, wexp, ro,
):
    step = pl.program_id(0)
    steps = pl.num_programs(0)
    block, heads, values, keys = mem_ref.shape
    span, _, seqs = pi_ref.shape
    rows = seqs * span
    lanes = 128
    iota = lambda shape, d: lax.broadcasted_iota(jnp.int32, shape, d)

    @pl.when(step == 0)
    def _():
        spread = (iota((seqs, rows), 0) == iota((seqs, rows), 1) // span)
        expand = spread.astype(F32)
        lane_pos = iota((span, rows), 1) % span == iota((span, rows), 0)
        dropped = iota((span, seqs), 0) >= acc_ref[...]
        ro[...] = jnp.zeros_like(ro)
        single = [
            jnp.where(lane_pos, ref[h : h + 1, :], 0.0)
            for h in range(heads)
            for ref in (gi_ref, gf_ref)
        ]
        compact = nt(jnp.concatenate(single, axis=0), expand, HIGHEST)
        position = iota((2 * span, seqs), 0)
        stack, decays = [], []
        for h in range(heads):
            stab = stab_ref[h : h + 1, :]
            f = jnp.where(dropped, 0.0, pf_ref[:, h, :])
            i = jnp.where(dropped, FAR_NEGATIVE, pi_ref[:, h, :])
            new_i = compact[2 * h * span : (2 * h + 1) * span]
            new_f = compact[(2 * h + 1) * span : (2 * h + 2) * span]
            ni_ref[:, h, :] = new_i
            nf_ref[:, h, :] = new_f
            total = []
            for j in range(span):
                total.append(f[j : j + 1] + total[-1] if total else f[0:1])
            e = total[-1]
            for j in range(span):
                total.append(total[-1] + new_f[j : j + 1])
            run_prev = jnp.concatenate(total[:span], axis=0)
            run_all = jnp.concatenate(total, axis=0)
            in_all = jnp.concatenate([i, new_i], axis=0)
            u = e - run_prev + i
            ns = jnp.maximum(e + stab, jnp.max(u, axis=0, keepdims=True))
            ns_ref[h : h + 1, :] = ns
            decays.append(jnp.exp(e + stab - ns))
            stack += [jnp.exp(u - ns), jnp.zeros((8 - span, seqs), F32)]
            for t in range(span):
                latest = total[span + t]
                d = jnp.where(position <= span + t, latest - run_all + in_all, FAR_NEGATIVE)
                g = latest + stab
                top = jnp.maximum(jnp.max(d, axis=0, keepdims=True), g)
                pad = jnp.zeros((16 - 2 * span - 2, seqs), F32)
                stack += [jnp.exp(d - top), jnp.exp(g - top), jnp.exp(-top), pad]
        wide = nn(jnp.concatenate(stack, axis=0), expand, HIGHEST)
        decays = jnp.concatenate(decays + [jnp.zeros((8 - heads, seqs), F32)], axis=0).T
        each = 8 + 16 * span
        for h in range(heads):
            base = h * each
            share_row = jnp.sum(
                jnp.where(lane_pos, wide[base : base + span], 0.0), axis=0, keepdims=True
            )
            old = pk_ref[:, h * keys : (h + 1) * keys]
            odd = (iota((rows, keys), 0) // span) % 2
            kps[h] = jnp.concatenate(
                [jnp.where(odd == p, old, jnp.zeros_like(old)) for p in range(2)], axis=1
            )
            part = slice(h * values, (h + 1) * values)
            vts[part, :] = (pv_ref[part, :].astype(F32) * share_row).astype(BF16)
            full = jnp.broadcast_to(decays[:, h : h + 1], (seqs, keys))
            dfull[h] = full
            mixed = jnp.where(spread, share_row, 0.0).astype(BF16)
            nn_ref[:, h, :] = full * nrm_ref[:, h, :] + nn(mixed, old)
            gathered = jnp.zeros((16, rows), F32)
            for t in range(span):
                at = base + 8 + 16 * t
                gathered = jnp.where(
                    iota((16, rows), 1) % span == t, wide[at : at + 16], gathered
                )
            wexp[h] = gathered

    first = step * block
    start = pl.multiple_of((first * span) // lanes * lanes, lanes)
    half = pl.ds(start, lanes)
    pair = ((iota((values, lanes), 1) + start) // span - first) // 2
    parity = (iota((keys, lanes), 1) // span) % 2
    for h in range(heads):
        part = slice(h * values, (h + 1) * values)
        memory = [mem_ref[s, h] for s in range(block)]
        packed = jnp.concatenate(
            [
                jnp.concatenate([memory[s].astype(BF16), memory[s + 1].astype(BF16)], axis=1)
                for s in range(0, block, 2)
            ],
            axis=0,
        )
        query = q_ref[h * keys : (h + 1) * keys, half]
        none = jnp.zeros_like(query)
        both = jnp.concatenate([jnp.where(parity == p, query, none) for p in range(2)], axis=0)
        read = nn(packed, both)
        total = ro[part, half]
        for s in range(block // 2):
            total = jnp.where(pair == s, read[s * values : (s + 1) * values], total)
        ro[part, half] = total
        shared = vts[part, half]
        zero = jnp.zeros_like(shared)
        left = jnp.concatenate(
            [jnp.where(pair == s, shared, zero) for s in range(block // 2)], axis=0
        )
        update = nn(left, kps[h, half, :])
        for s in range(block):
            at = s // 2 * values
            nm_ref[s, h] = (
                dfull[h, pl.ds(first + s, 1), :] * memory[s]
                + update[at : at + values, s % 2 * keys : (s % 2 + 1) * keys]
            )

    @pl.when(step == steps - 1)
    def _():
        same = iota((rows, rows), 0) // span == iota((rows, rows), 1) // span
        spread = iota((seqs, rows), 0) == iota((seqs, rows), 1) // span
        q = q_ref[...]
        owner = iota(q.shape, 0) // keys

        z = lax.axis_index("kv")
        gains = gain_ref[:, :values]
        for i in range(1, gain_ref.shape[1] // values):
            gains = jnp.where(
                lax.axis_index("tp") == i, gain_ref[:, i * values : (i + 1) * values], gains
            )
        local = gains[:heads]
        for i in range(1, gain_ref.shape[0] // heads):
            local = jnp.where(z == i, gains[i * heads : (i + 1) * heads], local)

        columns = jnp.concatenate([local, jnp.zeros((8 - heads, values), F32)], axis=0).T

        def tile(w):
            w = jnp.concatenate([w] * (8 // span), axis=0)
            return jnp.broadcast_to(w[None], (rows // 8, 8, rows)).reshape(rows, rows)

        for h in range(heads):
            part = slice(h * values, (h + 1) * values)
            only = jnp.where(owner == h, q, jnp.zeros_like(q))
            w = wexp[h]
            w_prev = jnp.where(same, tile(w[:span]) * nn(pk_ref[...], only), 0.0)
            w_new = jnp.where(same, tile(w[span : 2 * span]) * nn(k_ref[...], only), 0.0)
            carry = w[2 * span : 2 * span + 1]
            floor = w[2 * span + 1 : 2 * span + 2]
            top = nn(pv_ref[part, :], w_prev.astype(BF16)) + nn(v_ref[part, :], w_new.astype(BF16))
            top = top + carry * ro[part, :]
            nq = nn(nrm_ref[:, h, :].astype(BF16), q_ref[h * keys : (h + 1) * keys, :])
            nq = jnp.sum(jnp.where(spread, nq, 0.0), axis=0, keepdims=True)
            under = jnp.sum(w_prev + w_new, axis=0, keepdims=True) + carry * nq
            cell = top / jnp.maximum(jnp.abs(under), floor)
            sq_ref[h : h + 1, :] = jnp.sum(cell * cell, axis=0, keepdims=True)
            gain = columns[:, h : h + 1]
            g_ref[part, :] = (jax.nn.sigmoid(og_ref[part, :]) * cell * gain).astype(BF16)


def output_kernel(
    n, full_values, halves,
    g_ref, sq_ref, own_hbm, other_hbm,
    y_ref,
    g_in, sq_in, both, from_low, from_high, to_high, to_low, total, w_ref,
    load_sem,
    side_send, side_recv, up_send, up_recv, down_send, down_recv,
):
    z = lax.axis_index("kv")
    c = lax.axis_index("tp")
    channels = g_ref.shape[0]
    width = y_ref.shape[2]
    loads = []
    for d in range(n):
        col = pl.multiple_of((2 * d + c) * width, width)
        loads += [
            pltpu.make_async_copy(
                own_hbm.at[:, pl.ds(col, width)], w_ref.at[d, pl.ds(0, channels)],
                load_sem.at[2 * d],
            ),
            pltpu.make_async_copy(
                other_hbm.at[d], w_ref.at[d, pl.ds(channels, channels)], load_sem.at[2 * d + 1]
            ),
        ]
    for load in loads:
        load.start()
    enter(n, z, c)
    side = {"tp": 1 - c}
    swaps = [
        pltpu.make_async_remote_copy(
            src_ref=src, dst_ref=dst, send_sem=side_send.at[i], recv_sem=side_recv.at[i],
            device_id=side, device_id_type=MESH,
        )
        for i, (src, dst) in enumerate(((g_ref, g_in), (sq_ref, sq_in)))
    ]
    for swap in swaps:
        swap.start()
    for swap in swaps:
        swap.wait_recv()
    inv = lax.rsqrt((sq_ref[...] + sq_in[...]) / full_values + EPS)
    heads = sq_ref.shape[0]
    values = channels // heads
    for i, src in enumerate((g_ref, g_in)):
        scaled = jnp.concatenate(
            [
                src[h * values : (h + 1) * values, :].astype(F32) * inv[h : h + 1, :]
                for h in range(heads)
            ],
            axis=0,
        )
        both[:, i * channels : (i + 1) * channels] = scaled.T.astype(BF16)

    for load in loads:
        load.wait()
    height = both.shape[0] // halves

    def partial(d, half):
        return nn(both[half * height : (half + 1) * height], w_ref[d])

    def upward(d, half):
        return pltpu.make_async_remote_copy(
            src_ref=to_high.at[d, half], dst_ref=from_low.at[d, half],
            send_sem=up_send.at[d, half], recv_sem=up_recv.at[d, half],
            device_id={"kv": z + 1}, device_id_type=MESH,
        )

    def downward(d, half):
        return pltpu.make_async_remote_copy(
            src_ref=to_low.at[d, half], dst_ref=from_high.at[d, half],
            send_sem=down_send.at[d, half], recv_sem=down_recv.at[d, half],
            device_id={"kv": z - 1}, device_id_type=MESH,
        )

    def step(i, carry):
        high = n - 1 - i + z
        low = i - (n - 1 - z)
        for half in range(halves):
            @pl.when((high > z) & (high <= n - 1))
            def _():
                term = partial(high, half)

                @pl.when(z == 0)
                def _():
                    to_high[high, half] = term.astype(BF16)

                @pl.when(z > 0)
                def _():
                    upward(high, half).wait_recv()
                    to_high[high, half] = (term + from_low[high, half].astype(F32)).astype(BF16)

                upward(high, half).start()

            @pl.when((low < z) & (low >= 0))
            def _():
                term = partial(low, half)

                @pl.when(z == n - 1)
                def _():
                    to_low[low, half] = term.astype(BF16)

                @pl.when(z < n - 1)
                def _():
                    downward(low, half).wait_recv()
                    to_low[low, half] = (term + from_high[low, half].astype(F32)).astype(BF16)

                downward(low, half).start()

        return carry

    lax.fori_loop(0, 2 * n - 2, step, 0)
    for half in range(halves):
        total[half] = partial(z, half)
    for half in range(halves):
        @pl.when(z > 0)
        def _():
            upward(z, half).wait_recv()
            total[half] += from_low[z, half].astype(F32)

        @pl.when(z < n - 1)
        def _():
            downward(z, half).wait_recv()
            total[half] += from_high[z, half].astype(F32)

    seqs, span, width = y_ref.shape
    y_ref[...] = total[...].reshape(seqs, span, width).astype(BF16)

    def drain(i, carry):
        for half in range(halves):
            @pl.when(i > z)
            def _():
                upward(i, half).wait_send()

            @pl.when(i < z)
            def _():
                downward(i, half).wait_send()

        return carry

    lax.fori_loop(0, n, drain, 0)
    for swap in swaps:
        swap.wait_send()


def shards(
    n, tokens, norm_gain, w_query, w_key, w_value, w_outgate, w_input, w_forget, forget_bias,
    head_gain, w_out, memory, normalizer, stabilizer, prev_keys, prev_values, prev_input,
    prev_forget, accepted,
):
    seqs, span, width = tokens.shape
    depth, heads, keys = w_query.shape
    values = w_value.shape[2]
    rows = seqs * span
    hk, hv = heads * keys, heads * values
    all_heads = w_input.shape[1]
    sds = jax.ShapeDtypeStruct
    vm = pl.BlockSpec(memory_space=pltpu.VMEM)
    hbm = pl.BlockSpec(memory_space=pl.ANY)
    flip = lambda w: w.transpose(1, 2, 0).reshape(-1, depth)

    halves = 2
    height = rows // halves
    channels = 2 * hk + 2 * hv + 2 * all_heads
    q, k, v, og, gi, gf, pk, pv, wout = pl.pallas_call(
        functools.partial(project_kernel, n, keys, halves),
        out_shape=[
            sds((hk, rows), BF16), sds((rows, hk), BF16), sds((hv, rows), BF16),
            sds((hv, rows), F32), sds((heads, rows), F32), sds((heads, rows), F32),
            sds((rows, hk), BF16), sds((hv, rows), BF16), sds((n, hv, width), BF16),
        ],
        in_specs=[vm, vm] + [hbm] * 6 + [vm, vm, vm, hbm],
        out_specs=[vm] * 8 + [hbm],
        scratch_shapes=[
            pltpu.VMEM((2 * n, halves, height, width), BF16),
            pltpu.VMEM((channels, depth), BF16),
            pltpu.VMEM((channels, rows), F32),
            pltpu.VMEM((rows, 128), F32),
            pltpu.SemaphoreType.DMA((6,)),
            pltpu.SemaphoreType.DMA((3, 2 * n, halves)),
            pltpu.SemaphoreType.DMA((2 * n, halves)),
            pltpu.SemaphoreType.DMA((n,)),
            pltpu.SemaphoreType.DMA((n,)),
        ],
        compiler_params=pltpu.CompilerParams(
            collective_id=0, has_side_effects=True, vmem_limit_bytes=VMEM_LIMIT
        ),
        name="project",
    )(
        tokens, norm_gain.reshape(1, depth),
        flip(w_query), flip(w_key), flip(w_value), flip(w_outgate),
        w_input.T, w_forget.T, forget_bias.reshape(1, all_heads), prev_keys, prev_values,
        w_out.reshape(hv, -1),
    )

    block = 8
    whole = lambda *shape: pl.BlockSpec(shape, lambda i: (0,) * len(shape))
    tile = pl.BlockSpec((block, heads, values, keys), lambda i: (i, 0, 0, 0))
    new_memory, new_normalizer, ns, ni, nf, g, sq = pl.pallas_call(
        recurrent_kernel,
        grid=(seqs // block,),
        out_shape=[
            sds(memory.shape, F32), sds(normalizer.shape, F32), sds((heads, seqs), F32),
            sds((span, heads, seqs), F32), sds((span, heads, seqs), F32),
            sds((hv, rows), BF16), sds((heads, rows), F32),
        ],
        in_specs=[
            whole(hk, rows), whole(rows, hk), whole(hv, rows), whole(hv, rows),
            whole(heads, rows), whole(heads, rows), whole(rows, hk), whole(hv, rows),
            whole(span, heads, seqs), whole(span, heads, seqs), whole(1, seqs),
            whole(heads, seqs), whole(seqs, heads, keys), whole(*head_gain.shape), tile,
        ],
        out_specs=[
            tile, whole(seqs, heads, keys), whole(heads, seqs), whole(span, heads, seqs),
            whole(span, heads, seqs), whole(hv, rows), whole(heads, rows),
        ],
        scratch_shapes=[
            pltpu.VMEM((hv, rows), BF16), pltpu.VMEM((heads, rows, 2 * keys), BF16),
            pltpu.VMEM((heads, seqs, keys), F32), pltpu.VMEM((heads, 16, rows), F32),
            pltpu.VMEM((hv, rows), F32),
        ],
        compiler_params=pltpu.CompilerParams(vmem_limit_bytes=VMEM_LIMIT),
        name="recurrent",
    )(
        q, k, v, og, gi, gf, pk, pv,
        prev_input.transpose(1, 2, 0), prev_forget.transpose(1, 2, 0),
        accepted.reshape(1, seqs), stabilizer.T, normalizer, head_gain, memory,
    )

    y = pl.pallas_call(
        functools.partial(output_kernel, n, values * 2, halves),
        out_shape=sds(tokens.shape, BF16),
        in_specs=[vm, vm, hbm, hbm],
        out_specs=vm,
        scratch_shapes=[pltpu.VMEM((hv, rows), BF16), pltpu.VMEM((heads, rows), F32)]
        + [pltpu.VMEM((rows, 2 * hv), BF16)]
        + [pltpu.VMEM((n, halves, height, width), BF16)] * 4
        + [pltpu.VMEM((halves, height, width), F32), pltpu.VMEM((n, 2 * hv, width), BF16)]
        + [pltpu.SemaphoreType.DMA((2 * n,))]
        + [pltpu.SemaphoreType.DMA((2,))] * 2
        + [pltpu.SemaphoreType.DMA((n, halves))] * 4,
        compiler_params=pltpu.CompilerParams(
            collective_id=1, has_side_effects=True, vmem_limit_bytes=VMEM_LIMIT
        ),
        name="output",
    )(g, sq, w_out.reshape(hv, -1), wout)

    return (
        y,
        new_memory,
        new_normalizer,
        ns.T,
        k.reshape(seqs, span, heads, keys),
        v.T.reshape(seqs, span, heads, values),
        ni.transpose(2, 0, 1),
        nf.transpose(2, 0, 1),
    )


def solution(mesh):
    return jax.shard_map(
        functools.partial(shards, mesh.shape["kv"]),
        mesh=mesh,
        in_specs=(
            P(("grp", "dp"), None, ("kv", "tp")),
            P(),
            P(None, "kv", None),
            P(None, "kv", None),
            P(None, "kv", "tp"),
            P(None, "kv", "tp"),
            P(),
            P(),
            P(),
            P(),
            P("kv", "tp", None),
            P(("grp", "dp"), "kv", "tp", None),
            P(("grp", "dp"), "kv", None),
            P(("grp", "dp"), "kv"),
            P(("grp", "dp"), None, "kv", None),
            P(("grp", "dp"), None, "kv", "tp"),
            P(("grp", "dp"), None, "kv"),
            P(("grp", "dp"), None, "kv"),
            P(("grp", "dp")),
        ),
        out_specs=(
            P(("grp", "dp"), None, ("kv", "tp")),
            P(("grp", "dp"), "kv", "tp", None),
            P(("grp", "dp"), "kv", None),
            P(("grp", "dp"), "kv"),
            P(("grp", "dp"), None, "kv", None),
            P(("grp", "dp"), None, "kv", "tp"),
            P(("grp", "dp"), None, "kv"),
            P(("grp", "dp"), None, "kv"),
        ),
        check_vma=False,
    )
```
